512 devices in a mesh: sp: 16 (over z), tp: 4 (over y), dp: 8 (over x, core).
Axes of the slice: x: 4, y: 4, z: 16, core: 2. Of those that a mesh axis runs over, the one named last changes fastest.
Arguments:
- latent: bfloat16 [8, 6144, 2048], P('dp', 'sp'), may hold values from -6 to 6
- conditioning: bfloat16 [8, 2048], P(None, 'sp'), may hold values from -6 to 6
- context_cond: bfloat16 [2048], P('sp'), may hold values from -6 to 6
- modulation: bfloat16 [3, 2048, 2048], P(None, 'sp', ('tp', 'dp')), may hold values from -4.2426407 to 4.2426407
- context: bfloat16 [8, 1024, 2048], P('dp', 'sp'), may hold values from -6 to 6
- query_weight: bfloat16 [2048, 1024], P(None, 'tp'), may hold values from -2.1213203 to 2.1213203
- key_projection: bfloat16 [2048, 256], P(None, 'tp'), may hold values from -0.13258252 to 0.13258252
- value_projection: bfloat16 [2048, 256], P(None, 'tp'), may hold values from -0.125 to 0.125
- out_weight: bfloat16 [1024, 2048], P(None, 'tp'), may hold values from -0.1875 to 0.1875
- sink_head_logit: float32 [16], P('tp'), may hold values from 5 to 7.5
- prefix_logit_bias: float32 [16], P('tp'), may hold values from -2.5 to -1
Outputs:
- updated: float32 [8, 6144, 2048], P('dp', 'sp', 'tp')
The draws below stay inside these ranges and needn't reach their ends.
All inputs are finite; a program needn't handle non-finite values.
Results may differ from the reference program's by a relative error of at most 0.0073.
Values may be sent and summed in bfloat16 or wider, within the bound.
No kernel may reach another device: no remote copies, remote signals or barrier semaphores. Data moves between devices by JAX's collectives and lax.ppermute only.
A program may use at most 64 MiB of HBM per device.

```python
import jax
import jax.numpy as jnp
from jax import lax

MODEL_WIDTH = 2048
QUERY_HEADS = 16
KEY_VALUE_HEADS = 4
HEAD_SIZE = 64
GRID_W = 64
WINDOW_REACH = 128
SAMPLES = 8
LATENT_TOKENS = 6144
CONTEXT_TOKENS = 1024


def key_lookup_table(key):
    clip_bound = 6.0 * MODEL_WIDTH ** (-0.5)
    sampled_draws = jax.random.normal(jax.random.fold_in(key, 71), (MODEL_WIDTH, KEY_VALUE_HEADS * HEAD_SIZE), jnp.float32) * MODEL_WIDTH ** (-0.5)
    return jnp.clip(sampled_draws, -clip_bound, clip_bound)


def draw_key_projection(key, part):
    return key_lookup_table(key).astype(jnp.bfloat16)


def draw_query_weight(key, part):
    query_key = jax.random.fold_in(key, 72)
    clip_bound = 6.0 * MODEL_WIDTH ** (-0.5)
    sampled_draws = jax.random.normal(query_key, (MODEL_WIDTH, QUERY_HEADS * HEAD_SIZE), jnp.float32) * MODEL_WIDTH ** (-0.5)
    sampled_draws = jnp.clip(sampled_draws, -clip_bound, clip_bound)
    return sampled_draws.astype(jnp.bfloat16)


def draw_modulation(key, part):
    mod_key = jax.random.fold_in(key, 73)
    sampled_draws = jnp.clip(jax.random.normal(mod_key, (3, MODEL_WIDTH, MODEL_WIDTH), jnp.float32), -6.0, 6.0)
    boost = jnp.array([1.0, 1.0, 32.0], jnp.float32)[:, None, None]
    return (sampled_draws * boost * MODEL_WIDTH ** (-0.5)).astype(jnp.bfloat16)


def block_scale(rng, extent, cuts, low, largest):
    def one(position, shards_of):
        draws = jax.random.uniform(jax.random.fold_in(jax.random.fold_in(rng, 6), position), (shards_of,), jnp.float32, low / len(cuts), largest / len(cuts))
        return jnp.repeat(jnp.exp(draws), extent[position] // shards_of).reshape((-1,) + (1,) * (len(extent) - position - 1))

    factor_of = one(*cuts[0])
    for cut in cuts[1:]:
        factor_of = factor_of * one(*cut)
    return factor_of


def bell_draw(key, shape, deviation, limit, split=(), kind=jnp.bfloat16):
    drawn = jax.random.normal(key, shape, jnp.float32) * deviation
    if len(split) > 0:
        drawn = block_scale(key, shape, split, -0.22, 0.18) * drawn
    return jnp.clip(drawn, min=-limit, max=limit).astype(kind)


def setup_inputs(seed: int = 0) -> dict:
    key_list = jax.random.split(jax.random.key(seed), 12)
    latent = bell_draw(key_list[0], (SAMPLES, LATENT_TOKENS, MODEL_WIDTH), 1.0, 6.0, ((0, 8), (1, 16)))
    conditioning = bell_draw(key_list[1], (SAMPLES, MODEL_WIDTH), 1.0, 6.0, ((1, 16),))
    context_cond = bell_draw(key_list[2], (MODEL_WIDTH,), 1.0, 6.0, ((0, 16),))
    modulation = draw_modulation(jax.random.fold_in(key_list[11], 71), 0)
    context = bell_draw(key_list[4], (SAMPLES, CONTEXT_TOKENS, MODEL_WIDTH), 1.0, 6.0, ((0, 8), (1, 16)))
    query_weight = draw_query_weight(jax.random.fold_in(key_list[11], 71), 0)
    key_projection = draw_key_projection(jax.random.fold_in(key_list[11], 71), 0)
    value_projection = bell_draw(key_list[7], (MODEL_WIDTH, KEY_VALUE_HEADS * HEAD_SIZE), MODEL_WIDTH ** -0.5, 0.125, ((1, 4),))
    out_weight = bell_draw(key_list[8], (QUERY_HEADS * HEAD_SIZE, MODEL_WIDTH), (QUERY_HEADS * HEAD_SIZE) ** -0.5, 0.1875, ((1, 4),))
    sink_head_logit = jnp.clip(5.0 + 2.5 * jax.random.uniform(key_list[9], (QUERY_HEADS,), jnp.float32) ** block_scale(key_list[9], (QUERY_HEADS,), ((0, 4),), -0.2, 0.2), 5.0, 7.5)
    prefix_logit_bias = jnp.clip(-2.5 + 1.5 * jax.random.uniform(key_list[10], (QUERY_HEADS,), jnp.float32) ** block_scale(key_list[10], (QUERY_HEADS,), ((0, 4),), -0.2, 0.2), -2.5, -1.0)
    return {"latent": latent, "conditioning": conditioning, "context_cond": context_cond, "modulation": modulation, "context": context, "query_weight": query_weight, "key_projection": key_projection, "value_projection": value_projection, "out_weight": out_weight, "sink_head_logit": sink_head_logit, "prefix_logit_bias": prefix_logit_bias}


NORM_EPSILON = 1e-06
ROTARY_BASE = 10000.0
MASKED = -1e+30

def layer_norm(tok_rows):
    vectors = tok_rows.astype(jnp.float32)
    centre = lax.optimization_barrier(jnp.mean(vectors, axis=-1, keepdims=True))
    spread = lax.optimization_barrier(jnp.mean(jnp.square(vectors - centre), axis=-1, keepdims=True))
    return (vectors - centre) * lax.rsqrt(spread + NORM_EPSILON)

def turn_half(segment, token_positions):
    half_width = segment.shape[-1]
    quarter = half_width // 2
    frequency = ROTARY_BASE ** (-jnp.arange(0, half_width, 2, dtype=jnp.float32) / half_width)
    angles = token_positions.astype(jnp.float32)[:, None] * frequency[None, :]
    cosine = jnp.cos(angles)[:, None, :]
    sine_table = jnp.sin(angles)[:, None, :]
    leading = segment[..., :quarter]
    trailing = segment[..., quarter:]
    return jnp.concatenate([leading * cosine - trailing * sine_table, trailing * cosine + leading * sine_table], axis=-1)

def apply_rotary(head_rows, token_positions):
    half_width = head_rows.shape[-1] // 2
    return jnp.concatenate([turn_half(head_rows[..., :half_width], token_positions // GRID_W), turn_half(head_rows[..., half_width:], token_positions % GRID_W)], axis=-1)

def rounded_length(array):
    return lax.optimization_barrier(array.astype(jnp.bfloat16))

def reference(latent, conditioning, context_cond, modulation, context, query_weight, key_projection, value_projection, out_weight, sink_head_logit, prefix_logit_bias):
    cond_rows = jnp.concatenate([conditioning, context_cond[None, :]], axis=0)
    activated = jax.nn.silu(cond_rows.astype(jnp.float32)).astype(jnp.bfloat16)
    mod_all = jnp.stack([jnp.dot(activated, modulation[index], preferred_element_type=jnp.float32) for index in range(3)])
    ctx_shift = mod_all[0, -1]
    ctx_scale = mod_all[1, -1]
    heads_per_group = QUERY_HEADS // KEY_VALUE_HEADS
    block_list = LATENT_TOKENS // WINDOW_REACH
    factor = HEAD_SIZE ** (-0.5)
    token_positions = jnp.arange(LATENT_TOKENS, dtype=jnp.int32)
    block_start = jnp.arange(block_list, dtype=jnp.int32)[:, None] * WINDOW_REACH
    query_pos = block_start + jnp.arange(WINDOW_REACH, dtype=jnp.int32)[None, :]
    key_pos = block_start - WINDOW_REACH + jnp.arange(3 * WINDOW_REACH, dtype=jnp.int32)[None, :]
    inside = (key_pos >= 0) & (key_pos < LATENT_TOKENS)
    valid = (jnp.abs(query_pos[:, :, None] - key_pos[:, None, :]) <= WINDOW_REACH) & inside[:, None, :]
    head_bias_rows = prefix_logit_bias.astype(jnp.float32).reshape(KEY_VALUE_HEADS, heads_per_group)[:, :, None, None]
    sink_head_rows = sink_head_logit.astype(jnp.float32).reshape(KEY_VALUE_HEADS, heads_per_group)[:, :, None, None]

    def one_sample(operands):
        sample_rows, sample_ctx, mod_shift, mod_scale, mod_gate = operands
        normalized_input = (layer_norm(sample_rows) * (1.0 + mod_scale) + mod_shift).astype(jnp.bfloat16)
        ctx_normed = (layer_norm(sample_ctx) * (1.0 + ctx_scale) + ctx_shift).astype(jnp.bfloat16)
        query_rows = rounded_length(apply_rotary(jnp.dot(normalized_input, query_weight, preferred_element_type=jnp.float32).reshape(LATENT_TOKENS, QUERY_HEADS, HEAD_SIZE), token_positions))
        key_token_rows = rounded_length(apply_rotary(jnp.dot(normalized_input, key_projection, preferred_element_type=jnp.float32).reshape(LATENT_TOKENS, KEY_VALUE_HEADS, HEAD_SIZE), token_positions))
        value_token_rows = rounded_length(jnp.dot(normalized_input, value_projection, preferred_element_type=jnp.float32)).reshape(LATENT_TOKENS, KEY_VALUE_HEADS, HEAD_SIZE)
        prefix_keys = rounded_length(jnp.dot(ctx_normed, key_projection, preferred_element_type=jnp.float32))
        prefix_keys = prefix_keys.reshape(CONTEXT_TOKENS, KEY_VALUE_HEADS, HEAD_SIZE).astype(jnp.float32)
        prefix_values = rounded_length(jnp.dot(ctx_normed, value_projection, preferred_element_type=jnp.float32))
        prefix_values = prefix_values.reshape(CONTEXT_TOKENS, KEY_VALUE_HEADS, HEAD_SIZE).astype(jnp.float32)
        padding_amount = ((WINDOW_REACH, WINDOW_REACH), (0, 0), (0, 0))
        key_padded_rows = jnp.pad(key_token_rows, padding_amount).reshape(block_list + 2, WINDOW_REACH, KEY_VALUE_HEADS, HEAD_SIZE)
        value_padded_rows = jnp.pad(value_token_rows, padding_amount).reshape(block_list + 2, WINDOW_REACH, KEY_VALUE_HEADS, HEAD_SIZE)
        window_keys = jnp.concatenate([key_padded_rows[:-2], key_padded_rows[1:-1], key_padded_rows[2:]], axis=1).astype(jnp.float32)
        window_values = jnp.concatenate([value_padded_rows[:-2], value_padded_rows[1:-1], value_padded_rows[2:]], axis=1).astype(jnp.float32)
        query_block_list = query_rows.reshape(block_list, WINDOW_REACH, KEY_VALUE_HEADS, heads_per_group, HEAD_SIZE).astype(jnp.float32)

        def one_block(pieces):
            block_queries, block_keys, block_values, block_valid = pieces
            win_scores = jnp.einsum('qkgd,jkd->kgqj', block_queries, block_keys) * factor
            win_scores = jnp.where(block_valid[None, None], win_scores, MASKED)
            ctx_scores = jnp.einsum('qkgd,ckd->kgqc', block_queries, prefix_keys) * factor + head_bias_rows
            sink_scores = jnp.broadcast_to(sink_head_rows, win_scores.shape[:-1] + (1,))
            probs = jax.nn.softmax(jnp.concatenate([win_scores, ctx_scores, sink_scores], axis=-1), axis=-1)
            win_probs = rounded_length(probs[..., :3 * WINDOW_REACH]).astype(jnp.float32)
            ctx_probs = rounded_length(probs[..., 3 * WINDOW_REACH:3 * WINDOW_REACH + CONTEXT_TOKENS]).astype(jnp.float32)
            summed = jnp.einsum('kgqj,jkd->qkgd', win_probs, block_values) + jnp.einsum('kgqc,ckd->qkgd', ctx_probs, prefix_values)
            return summed.astype(jnp.bfloat16)
        attended = lax.map(one_block, (query_block_list, window_keys, window_values, valid))
        attended = attended.reshape(LATENT_TOKENS, QUERY_HEADS * HEAD_SIZE)
        mixed = jnp.dot(attended, out_weight, preferred_element_type=jnp.float32)
        return sample_rows.astype(jnp.float32) + mod_gate * mixed
    return lax.map(one_sample, (latent, context, mod_all[0, :-1], mod_all[1, :-1], mod_all[2, :-1]))
```

```python
import functools

import jax
import jax.numpy as jnp
import numpy as np
from jax import lax
from jax.experimental import pallas as pl
from jax.experimental.pallas import tpu as pltpu
from jax.sharding import PartitionSpec as P

HEAD = 64
GRID_W = 64
REACH = 128
EPS = 1e-06
ROTARY_BASE = 10000.0
MASKED = -1e30
LANES = 128

f32 = jnp.float32
bf16 = jnp.bfloat16
VMEM = pl.BlockSpec(memory_space=pltpu.VMEM)
SMEM = pl.BlockSpec(memory_space=pltpu.SMEM)


def dot_nt(a, b):
    return lax.dot_general(a, b, (((1,), (1,)), ((), ())), preferred_element_type=f32)


def lanes_of(shape):
    return lax.broadcasted_iota(jnp.int32, shape, len(shape) - 1)


def call(kernel, out_shape, ins, scratch=()):
    return pl.pallas_call(
        kernel,
        out_shape=out_shape,
        in_specs=ins,
        out_specs=jax.tree.map(lambda _: VMEM, out_shape),
        scratch_shapes=list(scratch),
    )


def partial_kernel(cond_ref, ctx_ref, mod_ref, out_ref, rows, packed):
    samples = cond_ref.shape[0]
    rows[...] = jnp.zeros_like(rows)
    rows[0:samples, :] = cond_ref[...].astype(f32)
    rows[samples : samples + 1, :] = ctx_ref[...].astype(f32)
    v = rows[...]
    act = (v / (1.0 + jnp.exp(-v))).astype(bf16)
    shift = jnp.dot(act, mod_ref[0], preferred_element_type=f32)
    scale = jnp.dot(act, mod_ref[1], preferred_element_type=f32)
    gate = jnp.dot(act, mod_ref[2], preferred_element_type=f32)
    packed[...] = jnp.concatenate([shift, scale], axis=1)
    packed[9:13, :] = jnp.concatenate([gate[0:4], gate[4:8]], axis=1)
    out_ref[...] = jnp.broadcast_to(packed[...][None], out_ref.shape)


def rows_kernel(in_ref, out_ref, total):
    total[...] = jnp.sum(in_ref[...], axis=0)
    copies = out_ref.shape[0] // 8
    for d in range(8):
        gate = total[9 + d % 4 : 10 + d % 4, :]
        if d >= 4:
            gate = pltpu.roll(gate, 64, 1)
        for t in range(copies):
            out_ref[t * 8 + d, 0:1, :] = total[d : d + 1, :]
            out_ref[t * 8 + d, 1:2, :] = total[8:9, :]
            out_ref[t * 8 + d, 2:3, :] = gate
            out_ref[t * 8 + d, 3:4, :] = gate


def stats_kernel(x_ref, mean_ref, rstd_ref):
    width = x_ref.shape[1]
    step = 64

    def body(i, carry):
        at = pl.ds(pl.multiple_of(i * step, step), step)
        x = x_ref[at, :].astype(f32)
        mean = jnp.sum(x, axis=1, keepdims=True) * (1.0 / width)
        d = x - mean
        var = jnp.sum(d * d, axis=1, keepdims=True) * (1.0 / width)
        mean_ref[at, :] = jnp.broadcast_to(mean, (step, LANES))
        rstd_ref[at, :] = jnp.broadcast_to(lax.rsqrt(var + EPS), (step, LANES))
        return carry

    lax.fori_loop(0, x_ref.shape[0] // step, body, 0)


def stats(x):
    shape = jax.ShapeDtypeStruct((x.shape[0], LANES), f32)
    return call(stats_kernel, (shape, shape), [VMEM])(x)


def mod_tile(rows_ref, row, m):
    a = rows_ref[2 * m, row : row + 1, :]
    b = rows_ref[2 * m + 1, row : row + 1, :]
    low = lanes_of((1, LANES)) < 64
    shift = jnp.where(low, a, pltpu.roll(b, 64, 1))
    scale = jnp.where(low, pltpu.roll(a, 64, 1), b)
    return shift, 1.0 + scale


def modulate(x_ref, mean_ref, rstd_ref, rows_ref, row, out_ref, start):
    n = x_ref.shape[0]
    for m in range(x_ref.shape[1] // LANES):
        shift, scale = mod_tile(rows_ref, row, m)
        cols = slice(m * LANES, (m + 1) * LANES)
        x = x_ref[:, cols].astype(f32)
        y = (x - mean_ref[...]) * rstd_ref[...] * scale + shift
        out_ref[start : start + n, cols] = y.astype(bf16)


def ctx_kernel(x_ref, mean_ref, rstd_ref, rows_ref, wkv_ref, out_ref, normed):
    modulate(x_ref, mean_ref, rstd_ref, rows_ref, 1, normed, 0)
    kv = jnp.dot(normed[...], wkv_ref[...], preferred_element_type=f32).astype(bf16)
    out_ref[...] = jnp.broadcast_to(kv[None], out_ref.shape)


def turned(u, cos, sin):
    low = lanes_of(u.shape) % 32 < 16
    other = jnp.where(low, pltpu.roll(u, LANES - 16, 1), pltpu.roll(u, 16, 1))
    return u * cos + other * sin


def with_ones(kv):
    return jnp.where(lanes_of(kv.shape) < HEAD, jnp.ones_like(kv), kv)


def latent_kernel(
    x_ref, xb_ref, xa_ref, mean_ref, rstd_ref, hmean_ref, hrstd_ref, rows_ref, wq_ref, wkv_ref,
    cos_ref, sin_ref, q_ref, win_ref, normed, kv_s, ones_s,
):
    n = x_ref.shape[0]
    total = n + 2 * REACH
    modulate(xb_ref, hmean_ref.at[0:REACH], hrstd_ref.at[0:REACH], rows_ref, 0, normed, 0)
    modulate(x_ref, mean_ref, rstd_ref, rows_ref, 0, normed, REACH)
    modulate(
        xa_ref, hmean_ref.at[REACH : 2 * REACH], hrstd_ref.at[REACH : 2 * REACH], rows_ref, 0,
        normed, REACH + n,
    )
    cos, sin = cos_ref[...], sin_ref[...]
    key_lane = lanes_of((total, LANES)) < HEAD
    kv = jnp.dot(normed[...], wkv_ref[...], preferred_element_type=f32)
    kv = turned(kv, jnp.where(key_lane, cos, 1.0), jnp.where(key_lane, sin, 0.0)).astype(bf16)
    kv_s[...] = kv
    ones_s[...] = with_ones(kv)
    q = jnp.dot(normed[REACH : REACH + n, :], wq_ref[...], preferred_element_type=f32)
    low = lanes_of((n, LANES)) < HEAD
    own_cos, own_sin = cos_ref[REACH : REACH + n, :], sin_ref[REACH : REACH + n, :]
    for pair in range(q.shape[1] // LANES):
        u = turned(q[:, pair * LANES : (pair + 1) * LANES], own_cos, own_sin) * (HEAD ** -0.5)
        q_ref[2 * pair] = jnp.where(low, u, 0.0).astype(bf16)
        q_ref[2 * pair + 1] = jnp.where(low, pltpu.roll(u, HEAD, 1), 0.0).astype(bf16)
    heads = q_ref.shape[0]
    rows = heads * REACH
    blocks = n // REACH
    i = lax.broadcasted_iota(jnp.int32, (rows, 3 * REACH), 0) % REACH
    j = lanes_of((rows, 3 * REACH))
    near = (j >= i) & (j <= i + 2 * REACH)
    place = lax.axis_index("sp")
    first, last = place == 0, place == lax.axis_size("sp") - 1
    for b in range(blocks):
        qb = q_ref[:, b * REACH : (b + 1) * REACH, :].reshape(rows, LANES)
        s = dot_nt(qb, kv_s[b * REACH : (b + 3) * REACH, :])
        valid = near
        if b == 0:
            valid = valid & (j >= jnp.where(first, REACH, 0))
        if b == blocks - 1:
            valid = valid & (j < jnp.where(last, 2 * REACH, 3 * REACH))
        s = jnp.where(valid, s, MASKED)
        top = jnp.max(s, axis=1, keepdims=True)
        p = jnp.exp(s - top).astype(bf16)
        acc = jnp.dot(p, ones_s[b * REACH : (b + 3) * REACH, :], preferred_element_type=f32)
        acc = jnp.where(lanes_of(acc.shape) == 0, top, acc)
        win_ref[:, b * REACH : (b + 1) * REACH, :] = acc.reshape(heads, REACH, LANES)


def attend_kernel(q_ref, win_ref, ctx_ref, sink_ref, bias_ref, out_ref, ones_s, done):
    heads, n, _ = q_ref.shape
    kv = ctx_ref[...]
    ones_s[...] = with_ones(kv)
    step = REACH
    lane = lanes_of((step, LANES))
    for b in range(n // step):
        at = slice(b * step, (b + 1) * step)
        pieces = []
        for h in range(heads):
            bias, sink = bias_ref[h], sink_ref[h]
            s = dot_nt(q_ref[h, at, :], kv)
            win = win_ref[h, at, :]
            win_top = win[:, 0:1]
            top = jnp.maximum(
                jnp.maximum(jnp.max(s, axis=1, keepdims=True) + bias, win_top), sink
            )
            p = jnp.exp(s - (top - bias)).astype(bf16)
            acc = jnp.dot(p, ones_s[...], preferred_element_type=f32)
            acc = acc + win * jnp.exp(win_top - top)
            den = acc[:, 1:2] + jnp.exp(sink - top)
            acc = acc / den
            pieces.append(acc)
        for pair in range(heads // 2):
            even = pltpu.roll(pieces[2 * pair], HEAD, 1)
            both = jnp.where(lane < HEAD, even, pieces[2 * pair + 1])
            done[at, pair * LANES : (pair + 1) * LANES] = both.astype(bf16)
    out_ref[...] = jnp.broadcast_to(done[...][None], out_ref.shape)


def out_kernel(att_ref, w_ref, x_ref, rows_ref, out_ref):
    sources, n, width = att_ref.shape
    t = lax.axis_index("tp")
    mixed = jnp.dot(att_ref[0], w_ref[0:width, :], preferred_element_type=f32)
    for k in range(1, sources):
        mixed = mixed + jnp.dot(
            att_ref[k], w_ref[k * width : (k + 1) * width, :], preferred_element_type=f32
        )
    low = lanes_of((1, LANES)) < 64
    for m in range(out_ref.shape[1] // LANES):
        cols = slice(m * LANES, (m + 1) * LANES)
        a = rows_ref[t * 8 + 2 * m, 2:3, :]
        b = rows_ref[t * 8 + 2 * m + 1, 2:3, :]
        gate = jnp.where(low, a, pltpu.roll(b, 64, 1))
        out_ref[:, cols] = x_ref[:, cols].astype(f32) + gate * mixed[:, cols]


def rotary_tables(rows, start):
    lane = np.arange(LANES)
    freq = ROTARY_BASE ** (-np.arange(0, 32, 2, dtype=np.float32) / 32)
    freq = jnp.asarray(freq[lane % 16].astype(np.float32))
    by_row = jnp.asarray(lane % 64 < 32)
    sign = jnp.asarray(np.where(lane % 32 < 16, -1.0, 1.0).astype(np.float32))
    position = start + jnp.arange(rows, dtype=jnp.int32)
    row, col = position // GRID_W, position % GRID_W
    place = jnp.where(by_row[None, :], row[:, None], col[:, None]).astype(f32)
    angle = place * freq[None, :]
    return jnp.cos(angle), jnp.sin(angle) * sign[None, :]


def per_device(
    latent, conditioning, context_cond, modulation, context, query_weight, key_projection,
    value_projection, out_weight, sink_head_logit, prefix_logit_bias,
):
    sp, tp = lax.axis_size("sp"), lax.axis_size("tp")
    spread = tp * lax.axis_size("dp")
    x, ctx = latent[0], context[0]
    n = x.shape[0]
    partial = call(
        partial_kernel,
        jax.ShapeDtypeStruct((sp, 16, LANES), f32),
        [VMEM] * 3,
        [pltpu.VMEM((16, LANES), f32), pltpu.VMEM((16, LANES), f32)],
    )(conditioning, context_cond[None, :], modulation)
    with jax.named_scope("sums"):
        partials = lax.all_to_all(partial, "sp", 0, 0, tiled=True)
    up = [(i, i + 1) for i in range(sp - 1)]
    down = [(i + 1, i) for i in range(sp - 1)]
    with jax.named_scope("halo"):
        before = lax.ppermute(x[n - REACH :], "sp", up)
        after = lax.ppermute(x[:REACH], "sp", down)
    mean, rstd = stats(x)
    cmean, crstd = stats(ctx)
    wkv = jnp.concatenate([key_projection, value_projection], axis=1)
    start = lax.axis_index("sp") * n - REACH
    cos, sin = rotary_tables(n + 2 * REACH, start)
    send = call(
        rows_kernel,
        jax.ShapeDtypeStruct((spread, 4, LANES), f32),
        [VMEM],
        [pltpu.VMEM((16, LANES), f32)],
    )(partials)
    with jax.named_scope("spread"):
        rows = lax.all_to_all(send, ("tp", "dp"), 0, 0, tiled=True)
    hmean, hrstd = stats(jnp.concatenate([before, after], axis=0))
    ctx_kv = call(
        ctx_kernel,
        jax.ShapeDtypeStruct((sp, ctx.shape[0], LANES), bf16),
        [VMEM] * 5,
        [pltpu.VMEM(ctx.shape, bf16)],
    )(ctx, cmean, crstd, rows, wkv)
    with jax.named_scope("context"):
        ctx_all = lax.all_to_all(ctx_kv, "sp", 0, 0, tiled=True).reshape(-1, LANES)
    heads = query_weight.shape[1] // HEAD
    total = n + 2 * REACH
    q, win = call(
        latent_kernel,
        (
            jax.ShapeDtypeStruct((heads, n, LANES), bf16),
            jax.ShapeDtypeStruct((heads, n, LANES), f32),
        ),
        [VMEM] * 12,
        [
            pltpu.VMEM((total, x.shape[1]), bf16),
            pltpu.VMEM((total, LANES), bf16),
            pltpu.VMEM((total, LANES), bf16),
        ],
    )(x, before, after, mean, rstd, hmean, hrstd, rows, query_weight, wkv, cos, sin)
    attended = call(
        attend_kernel,
        jax.ShapeDtypeStruct((tp, n, heads * HEAD), bf16),
        [VMEM] * 3 + [SMEM] * 2,
        [pltpu.VMEM(ctx_all.shape, bf16), pltpu.VMEM((n, heads * HEAD), bf16)],
    )(q, win, ctx_all, sink_head_logit, prefix_logit_bias)
    with jax.named_scope("heads"):
        every = lax.all_to_all(attended, "tp", 0, 0, tiled=True)
    cols = out_weight.shape[1]
    own = lax.dynamic_slice_in_dim(x, lax.axis_index("tp") * cols, cols, 1)
    out = call(out_kernel, jax.ShapeDtypeStruct((n, cols), f32), [VMEM] * 4)(
        every, out_weight, own, rows
    )
    return out[None]


def solution(mesh):
    placed = (
        P("dp", "sp", None),
        P(None, "sp"),
        P("sp"),
        P(None, "sp", ("tp", "dp")),
        P("dp", "sp", None),
        P(None, "tp"),
        P(None, "tp"),
        P(None, "tp"),
        P(None, "tp"),
        P("tp"),
        P("tp"),
    )
    return jax.shard_map(
        per_device, mesh=mesh, in_specs=placed, out_specs=P("dp", "sp", "tp"), check_vma=False
    )
```

```python
import functools

import jax
import jax.numpy as jnp
import numpy as np
from jax import lax
from jax.experimental import pallas as pl
from jax.experimental.pallas import tpu as pltpu
from jax.sharding import PartitionSpec as P

HEAD = 64
GRID_W = 64
REACH = 128
EPS = 1e-06
ROTARY_BASE = 10000.0
MASKED = -1e30
LANES = 128

f32 = jnp.float32
bf16 = jnp.bfloat16
VMEM = pl.BlockSpec(memory_space=pltpu.VMEM)
SMEM = pl.BlockSpec(memory_space=pltpu.SMEM)
ANY = pl.BlockSpec(memory_space=pl.ANY)


def dot_nt(a, b):
    return lax.dot_general(a, b, (((1,), (1,)), ((), ())), preferred_element_type=f32)


def lanes_of(shape):
    return lax.broadcasted_iota(jnp.int32, shape, len(shape) - 1)


def call(kernel, out_shape, ins, scratch=(), mib=8):
    return pl.pallas_call(
        kernel,
        out_shape=out_shape,
        in_specs=ins,
        out_specs=jax.tree.map(lambda _: VMEM, out_shape),
        scratch_shapes=list(scratch),
        compiler_params=pltpu.CompilerParams(vmem_limit_bytes=mib << 20),
    )


def partial_kernel(cond_ref, ctx_ref, mod_ref, out_ref, rows, packed):
    samples = cond_ref.shape[0]
    rows[...] = jnp.zeros_like(rows)
    rows[0:samples, :] = cond_ref[...].astype(f32)
    rows[samples : samples + 1, :] = ctx_ref[...].astype(f32)
    v = rows[...]
    act = (v / (1.0 + jnp.exp(-v))).astype(bf16)
    shift = dot_nt(act, mod_ref[0])
    scale = dot_nt(act, mod_ref[1])
    gate = dot_nt(act, mod_ref[2])
    packed[...] = jnp.concatenate([shift, scale], axis=1)
    packed[9:13, :] = jnp.concatenate([gate[0:4], gate[4:8]], axis=1)
    out_ref[...] = jnp.broadcast_to(packed[...][None], out_ref.shape)


def rows_kernel(in_ref, *refs):
    out_ref, total = refs[-2:]
    total[...] = jnp.sum(in_ref[...], axis=0)
    copies = out_ref.shape[0] // 8
    for d in range(8):
        gate = total[9 + d % 4 : 10 + d % 4, :]
        if d >= 4:
            gate = pltpu.roll(gate, 64, 1)
        for t in range(copies):
            out_ref[t * 8 + d, 0:1, :] = total[d : d + 1, :]
            out_ref[t * 8 + d, 1:2, :] = total[8:9, :]
            out_ref[t * 8 + d, 2:3, :] = gate
            out_ref[t * 8 + d, 3:4, :] = gate


def stats_of(x_ref, mean_ref, rstd_ref):
    width = x_ref.shape[1]
    step = 64

    def body(i, carry):
        at = pl.ds(pl.multiple_of(i * step, step), step)
        x = x_ref[at, :].astype(f32)
        mean = jnp.sum(x, axis=1, keepdims=True) * (1.0 / width)
        d = x - mean
        var = jnp.sum(d * d, axis=1, keepdims=True) * (1.0 / width)
        mean_ref[at, :] = jnp.broadcast_to(mean, (step, LANES))
        rstd_ref[at, :] = jnp.broadcast_to(lax.rsqrt(var + EPS), (step, LANES))
        return carry

    lax.fori_loop(0, x_ref.shape[0] // step, body, 0)


def stats_kernel(x_ref, c_ref, mean_ref, rstd_ref, cmean_ref, crstd_ref):
    stats_of(x_ref, mean_ref, rstd_ref)
    stats_of(c_ref, cmean_ref, crstd_ref)


def mod_tile(rows_ref, row, m):
    a = rows_ref[2 * m, row : row + 1, :]
    b = rows_ref[2 * m + 1, row : row + 1, :]
    low = lanes_of((1, LANES)) < 64
    shift = jnp.where(low, a, pltpu.roll(b, 64, 1))
    scale = jnp.where(low, pltpu.roll(a, 64, 1), b)
    return shift, 1.0 + scale


def modulate(x_ref, mean_ref, rstd_ref, rows_ref, row, out_ref, start):
    n = x_ref.shape[0]
    for m in range(x_ref.shape[1] // LANES):
        shift, scale = mod_tile(rows_ref, row, m)
        cols = slice(m * LANES, (m + 1) * LANES)
        x = x_ref[:, cols].astype(f32)
        y = (x - mean_ref[...]) * rstd_ref[...] * scale + shift
        out_ref[start : start + n, cols] = y.astype(bf16)


def ctx_kernel(x_ref, mean_ref, rstd_ref, rows_ref, wkv_ref, out_ref, normed):
    modulate(x_ref, mean_ref, rstd_ref, rows_ref, 1, normed, 0)
    kv = dot_nt(normed[...], wkv_ref[...]).astype(bf16)
    out_ref[...] = jnp.broadcast_to(kv[None], out_ref.shape)


def turned(u, cos, sin):
    low = lanes_of(u.shape) % 32 < 16
    other = jnp.where(low, pltpu.roll(u, LANES - 16, 1), pltpu.roll(u, 16, 1))
    return u * cos + other * sin


def with_ones(kv):
    return jnp.where(lanes_of(kv.shape) < HEAD, jnp.ones_like(kv), kv)


def project_kernel(
    x_ref, mean_ref, rstd_ref, rows_ref, wq_ref, wkv_ref, cos_ref, sin_ref,
    q_ref, kv_ref, head_ref, tail_ref, normed,
):
    n = x_ref.shape[0]
    modulate(x_ref, mean_ref, rstd_ref, rows_ref, 0, normed, 0)
    cos, sin = cos_ref[...], sin_ref[...]
    low = lanes_of((n, LANES)) < HEAD
    kv = dot_nt(normed[...], wkv_ref[...])
    kv = turned(kv, jnp.where(low, cos, 1.0), jnp.where(low, sin, 0.0)).astype(bf16)
    kv_ref[...] = kv
    head_ref[...] = kv[0:REACH]
    tail_ref[...] = kv[n - REACH : n]
    q = jnp.dot(normed[...], wq_ref[...], preferred_element_type=f32)
    for pair in range(q.shape[1] // LANES):
        u = turned(q[:, pair * LANES : (pair + 1) * LANES], cos, sin) * (HEAD ** -0.5)
        q_ref[2 * pair] = jnp.where(low, u, 0.0).astype(bf16)
        q_ref[2 * pair + 1] = jnp.where(low, pltpu.roll(u, HEAD, 1), 0.0).astype(bf16)


def window_kernel(q_ref, kv_ref, before_ref, after_ref, win_ref, kv_s, ones_s):
    heads, n, _ = q_ref.shape
    kv_s[0:REACH, :] = before_ref[...]
    kv_s[REACH : REACH + n, :] = kv_ref[...]
    kv_s[REACH + n :, :] = after_ref[...]
    ones_s[...] = with_ones(kv_s[...])
    rows = heads * REACH
    blocks = n // REACH
    i = lax.broadcasted_iota(jnp.int32, (rows, 3 * REACH), 0) % REACH
    j = lanes_of((rows, 3 * REACH))
    near = (j >= i) & (j <= i + 2 * REACH)
    place = lax.axis_index("sp")
    first, last = place == 0, place == lax.axis_size("sp") - 1
    for b in range(blocks):
        qb = q_ref[:, b * REACH : (b + 1) * REACH, :].reshape(rows, LANES)
        s = dot_nt(qb, kv_s[b * REACH : (b + 3) * REACH, :])
        valid = near
        if b == 0:
            valid = valid & (j >= jnp.where(first, REACH, 0))
        if b == blocks - 1:
            valid = valid & (j < jnp.where(last, 2 * REACH, 3 * REACH))
        s = jnp.where(valid, s, MASKED)
        top = jnp.max(s, axis=1, keepdims=True)
        p = jnp.exp(s - top).astype(bf16)
        acc = jnp.dot(p, ones_s[b * REACH : (b + 3) * REACH, :], preferred_element_type=f32)
        acc = jnp.where(lanes_of(acc.shape) == 0, top, acc)
        win_ref[:, b * REACH : (b + 1) * REACH, :] = acc.reshape(heads, REACH, LANES)


def attend_kernel(q_ref, win_ref, ctx_ref, sink_ref, bias_ref, out_ref, ones_s, done):
    heads, n, _ = q_ref.shape
    kv = ctx_ref[...]
    ones_s[...] = with_ones(kv)
    step = REACH
    rows = heads * step
    lane = lanes_of((step, LANES))
    head = lax.broadcasted_iota(jnp.int32, (rows, 1), 0) // step
    bias, sink = jnp.zeros((rows, 1), f32), jnp.zeros((rows, 1), f32)
    for h in range(heads):
        bias = jnp.where(head == h, bias_ref[h], bias)
        sink = jnp.where(head == h, sink_ref[h], sink)
    for b in range(n // step):
        at = slice(b * step, (b + 1) * step)
        s = dot_nt(q_ref[:, at, :].reshape(rows, LANES), kv)
        win = win_ref[:, at, :].reshape(rows, LANES)
        win_top = win[:, 0:1]
        top = jnp.maximum(jnp.max(s, axis=1, keepdims=True) + bias, jnp.maximum(win_top, sink))
        p = jnp.exp(s - (top - bias)).astype(bf16)
        acc = jnp.dot(p, ones_s[...], preferred_element_type=f32)
        acc = acc + win * jnp.exp(win_top - top)
        den = acc[:, 1:2] + jnp.exp(sink - top)
        acc = (acc / den).reshape(heads, step, LANES)
        for pair in range(heads // 2):
            even = pltpu.roll(acc[2 * pair], HEAD, 1)
            both = jnp.where(lane < HEAD, even, acc[2 * pair + 1])
            done[at, pair * LANES : (pair + 1) * LANES] = both.astype(bf16)
    out_ref[...] = jnp.broadcast_to(done[...][None], out_ref.shape)


def out_kernel(att_ref, w_ref, x_ref, rows_ref, out_ref):
    sources, n, width = att_ref.shape
    t = lax.axis_index("tp")
    mixed = jnp.dot(att_ref[0], w_ref[0:width, :], preferred_element_type=f32)
    for k in range(1, sources):
        mixed = mixed + jnp.dot(
            att_ref[k], w_ref[k * width : (k + 1) * width, :], preferred_element_type=f32
        )
    low = lanes_of((1, LANES)) < 64
    for m in range(out_ref.shape[1] // LANES):
        cols = slice(m * LANES, (m + 1) * LANES)
        a = rows_ref[t * 8 + 2 * m, 2:3, :]
        b = rows_ref[t * 8 + 2 * m + 1, 2:3, :]
        gate = jnp.where(low, a, pltpu.roll(b, 64, 1))
        out_ref[:, cols] = x_ref[:, cols].astype(f32) + gate * mixed[:, cols]


def rotary_tables(rows, start):
    lane = np.arange(LANES)
    freq = ROTARY_BASE ** (-np.arange(0, 32, 2, dtype=np.float32) / 32)
    freq = jnp.asarray(freq[lane % 16].astype(np.float32))
    by_row = jnp.asarray(lane % 64 < 32)
    sign = jnp.asarray(np.where(lane % 32 < 16, -1.0, 1.0).astype(np.float32))
    position = start + jnp.arange(rows, dtype=jnp.int32)
    row, col = position // GRID_W, position % GRID_W
    place = jnp.where(by_row[None, :], row[:, None], col[:, None]).astype(f32)
    angle = place * freq[None, :]
    return jnp.cos(angle), jnp.sin(angle) * sign[None, :]


def per_device(
    latent, conditioning, context_cond, modulation, context, query_weight, key_projection,
    value_projection, out_weight, sink_head_logit, prefix_logit_bias,
):
    sp, tp = lax.axis_size("sp"), lax.axis_size("tp")
    spread = tp * lax.axis_size("dp")
    x, ctx = latent[0], context[0]
    n = x.shape[0]
    partial = call(
        partial_kernel,
        jax.ShapeDtypeStruct((sp, 16, LANES), f32),
        [VMEM] * 3,
        [pltpu.VMEM((16, LANES), f32), pltpu.VMEM((16, LANES), f32)],
        2,
    )(conditioning, context_cond[None, :], modulation.transpose(0, 2, 1))
    with jax.named_scope("sums"):
        partials = lax.all_to_all(partial, "sp", 0, 0, tiled=True)
    flat = jax.ShapeDtypeStruct((n, LANES), f32)
    cflat = jax.ShapeDtypeStruct((ctx.shape[0], LANES), f32)
    mean, rstd, cmean, crstd = call(stats_kernel, (flat, flat, cflat, cflat), [VMEM] * 2, (), 8)(
        x, ctx
    )
    wkv = jnp.concatenate([key_projection.T, value_projection.T], axis=0)
    cos, sin = rotary_tables(n, lax.axis_index("sp") * n)
    send = call(
        rows_kernel,
        jax.ShapeDtypeStruct((spread, 4, LANES), f32),
        [VMEM] + [ANY] * 4,
        [pltpu.VMEM((16, LANES), f32)],
        2,
    )(partials, cmean, wkv, cos, sin)
    with jax.named_scope("spread"):
        rows = lax.all_to_all(send, ("tp", "dp"), 0, 0, tiled=True)
    ctx_kv = call(
        ctx_kernel,
        jax.ShapeDtypeStruct((sp, ctx.shape[0], LANES), bf16),
        [VMEM] * 5,
        [pltpu.VMEM(ctx.shape, bf16)],
        4,
    )(ctx, cmean, crstd, rows, wkv)
    with jax.named_scope("context"):
        ctx_all = lax.all_to_all(ctx_kv, "sp", 0, 0, tiled=True).reshape(-1, LANES)
    heads = query_weight.shape[1] // HEAD
    edge = jax.ShapeDtypeStruct((REACH, LANES), bf16)
    q, kv, first, last = call(
        project_kernel,
        (
            jax.ShapeDtypeStruct((heads, n, LANES), bf16),
            jax.ShapeDtypeStruct((n, LANES), bf16),
            edge,
            edge,
        ),
        [VMEM] * 8,
        [pltpu.VMEM(x.shape, bf16)],
        12,
    )(x, mean, rstd, rows, query_weight, wkv, cos, sin)
    up = [(i, i + 1) for i in range(sp - 1)]
    down = [(i + 1, i) for i in range(sp - 1)]
    with jax.named_scope("halo"):
        before = lax.ppermute(last, "sp", up)
        after = lax.ppermute(first, "sp", down)
    wide = pltpu.VMEM((n + 2 * REACH, LANES), bf16)
    win = call(
        window_kernel,
        jax.ShapeDtypeStruct((heads, n, LANES), f32),
        [VMEM] * 4,
        [wide, wide],
        12,
    )(q, kv, before, after)
    attended = call(
        attend_kernel,
        jax.ShapeDtypeStruct((tp, n, heads * HEAD), bf16),
        [VMEM] * 3 + [SMEM] * 2,
        [pltpu.VMEM(ctx_all.shape, bf16), pltpu.VMEM((n, heads * HEAD), bf16)],
        16,
    )(q, win, ctx_all, sink_head_logit, prefix_logit_bias)
    with jax.named_scope("heads"):
        every = lax.all_to_all(attended, "tp", 0, 0, tiled=True)
    cols = out_weight.shape[1]
    own = lax.dynamic_slice_in_dim(x, lax.axis_index("tp") * cols, cols, 1)
    out = call(out_kernel, jax.ShapeDtypeStruct((n, cols), f32), [VMEM] * 4, (), 8)(
        every, out_weight, own, rows
    )
    return out[None]


def solution(mesh):
    placed = (
        P("dp", "sp", None),
        P(None, "sp"),
        P("sp"),
        P(None, "sp", ("tp", "dp")),
        P("dp", "sp", None),
        P(None, "tp"),
        P(None, "tp"),
        P(None, "tp"),
        P(None, "tp"),
        P("tp"),
        P("tp"),
    )
    return jax.shard_map(
        per_device, mesh=mesh, in_specs=placed, out_specs=P("dp", "sp", "tp"), check_vma=False
    )
```

```python
import functools

import jax
import jax.numpy as jnp
import numpy as np
from jax import lax
from jax.experimental import pallas as pl
from jax.experimental.pallas import tpu as pltpu
from jax.sharding import PartitionSpec as P

HEAD = 64
GRID_W = 64
REACH = 128
EPS = 1e-06
ROTARY_BASE = 10000.0
MASKED = -1e30
LANES = 128

f32 = jnp.float32
bf16 = jnp.bfloat16
VMEM = pl.BlockSpec(memory_space=pltpu.VMEM)
SMEM = pl.BlockSpec(memory_space=pltpu.SMEM)
ANY = pl.BlockSpec(memory_space=pl.ANY)


def in_hbm(x):
    return pltpu.with_memory_space_constraint(x, pltpu.HBM)


def dot_nt(a, b):
    return lax.dot_general(a, b, (((1,), (1,)), ((), ())), preferred_element_type=f32)


def lanes_of(shape):
    return lax.broadcasted_iota(jnp.int32, shape, len(shape) - 1)


def call(kernel, out_shape, ins, scratch=(), mib=8, out=VMEM):
    return pl.pallas_call(
        kernel,
        out_shape=out_shape,
        in_specs=ins,
        out_specs=jax.tree.map(lambda _: out, out_shape),
        scratch_shapes=list(scratch),
        compiler_params=pltpu.CompilerParams(vmem_limit_bytes=mib << 20),
    )


def partial_kernel(cond_ref, ctx_ref, mod_ref, out_ref, rows, packed):
    samples = cond_ref.shape[0]
    rows[...] = jnp.zeros_like(rows)
    rows[0:samples, :] = cond_ref[...].astype(f32)
    rows[samples : samples + 1, :] = ctx_ref[...].astype(f32)
    v = rows[...]
    act = (v / (1.0 + jnp.exp(-v))).astype(bf16)
    shift = dot_nt(act, mod_ref[0])
    scale = dot_nt(act, mod_ref[1])
    gate = dot_nt(act, mod_ref[2])
    packed[...] = jnp.concatenate([shift, scale], axis=1)
    packed[9:13, :] = jnp.concatenate([gate[0:4], gate[4:8]], axis=1)
    out_ref[...] = jnp.broadcast_to(packed[...].astype(bf16)[None], out_ref.shape)


def rows_kernel(in_ref, *refs):
    out_ref, total = refs[-2:]
    total[...] = jnp.sum(in_ref[...].astype(f32), axis=0)
    copies = out_ref.shape[0] // 8
    for d in range(8):
        gate = total[9 + d % 4 : 10 + d % 4, :]
        if d >= 4:
            gate = pltpu.roll(gate, 64, 1)
        for t in range(copies):
            out_ref[t * 8 + d, 0:1, :] = total[d : d + 1, :]
            out_ref[t * 8 + d, 1:2, :] = total[8:9, :]
            out_ref[t * 8 + d, 2:3, :] = gate
            out_ref[t * 8 + d, 3:4, :] = gate


def stats_of(x_ref, mean_ref, rstd_ref):
    width = x_ref.shape[1]
    step = 64

    def body(i, carry):
        at = pl.ds(pl.multiple_of(i * step, step), step)
        x = x_ref[at, :].astype(f32)
        mean = jnp.sum(x, axis=1, keepdims=True) * (1.0 / width)
        d = x - mean
        var = jnp.sum(d * d, axis=1, keepdims=True) * (1.0 / width)
        mean_ref[at, :] = jnp.broadcast_to(mean, (step, LANES))
        rstd_ref[at, :] = jnp.broadcast_to(lax.rsqrt(var + EPS), (step, LANES))
        return carry

    lax.fori_loop(0, x_ref.shape[0] // step, body, 0)


def stats_kernel(x_ref, c_ref, mean_ref, rstd_ref, cmean_ref, crstd_ref):
    stats_of(x_ref, mean_ref, rstd_ref)
    stats_of(c_ref, cmean_ref, crstd_ref)


def mod_tile(rows_ref, row, m):
    a = rows_ref[2 * m, row : row + 1, :]
    b = rows_ref[2 * m + 1, row : row + 1, :]
    low = lanes_of((1, LANES)) < 64
    shift = jnp.where(low, a, pltpu.roll(b, 64, 1))
    scale = jnp.where(low, pltpu.roll(a, 64, 1), b)
    return shift, 1.0 + scale


def modulate(x_ref, mean_ref, rstd_ref, rows_ref, row, out_ref, start):
    n = x_ref.shape[0]
    for m in range(x_ref.shape[1] // LANES):
        shift, scale = mod_tile(rows_ref, row, m)
        cols = slice(m * LANES, (m + 1) * LANES)
        x = x_ref[:, cols].astype(f32)
        y = (x - mean_ref[...]) * rstd_ref[...] * scale + shift
        out_ref[start : start + n, cols] = y.astype(bf16)


def ctx_kernel(x_ref, mean_ref, rstd_ref, rows_ref, wkv_ref, out_ref, normed):
    modulate(x_ref, mean_ref, rstd_ref, rows_ref, 1, normed, 0)
    kv = dot_nt(normed[...], wkv_ref[...]).astype(bf16)
    out_ref[...] = jnp.broadcast_to(kv[None], out_ref.shape)


def turned(u, cos, sin):
    low = lanes_of(u.shape) % 32 < 16
    other = jnp.where(low, pltpu.roll(u, LANES - 16, 1), pltpu.roll(u, 16, 1))
    return u * cos + other * sin


def with_ones(kv):
    return jnp.where(lanes_of(kv.shape) < HEAD, jnp.ones_like(kv), kv)


def project_kernel(
    x_ref, mean_ref, rstd_ref, rows_ref, wq_ref, wkv_ref, cos_ref, sin_ref,
    q_ref, kv_ref, head_ref, tail_ref, normed,
):
    n = x_ref.shape[0]
    modulate(x_ref, mean_ref, rstd_ref, rows_ref, 0, normed, 0)
    cos, sin = cos_ref[...], sin_ref[...]
    low = lanes_of((n, LANES)) < HEAD
    kv = dot_nt(normed[...], wkv_ref[...])
    kv = turned(kv, jnp.where(low, cos, 1.0), jnp.where(low, sin, 0.0)).astype(bf16)
    kv_ref[...] = kv
    head_ref[...] = kv[0:REACH]
    tail_ref[...] = kv[n - REACH : n]
    q = jnp.dot(normed[...], wq_ref[...], preferred_element_type=f32)
    for pair in range(q.shape[1] // LANES):
        u = turned(q[:, pair * LANES : (pair + 1) * LANES], cos, sin) * (HEAD ** -0.5)
        q_ref[2 * pair] = jnp.where(low, u, 0.0).astype(bf16)
        q_ref[2 * pair + 1] = jnp.where(low, pltpu.roll(u, HEAD, 1), 0.0).astype(bf16)


def window_kernel(q_ref, kv_ref, before_ref, after_ref, win_ref, kv_s, ones_s):
    heads, n, _ = q_ref.shape
    kv_s[0:REACH, :] = before_ref[...]
    kv_s[REACH : REACH + n, :] = kv_ref[...]
    kv_s[REACH + n :, :] = after_ref[...]
    ones_s[...] = with_ones(kv_s[...])
    rows = heads * REACH
    blocks = n // REACH
    i = lax.broadcasted_iota(jnp.int32, (rows, 3 * REACH), 0) % REACH
    j = lanes_of((rows, 3 * REACH))
    near = (j >= i) & (j <= i + 2 * REACH)
    place = lax.axis_index("sp")
    first, last = place == 0, place == lax.axis_size("sp") - 1
    for b in range(blocks):
        qb = q_ref[:, b * REACH : (b + 1) * REACH, :].reshape(rows, LANES)
        s = dot_nt(qb, kv_s[b * REACH : (b + 3) * REACH, :])
        valid = near
        if b == 0:
            valid = valid & (j >= jnp.where(first, REACH, 0))
        if b == blocks - 1:
            valid = valid & (j < jnp.where(last, 2 * REACH, 3 * REACH))
        s = jnp.where(valid, s, MASKED)
        top = jnp.max(s, axis=1, keepdims=True)
        p = jnp.exp(s - top).astype(bf16)
        acc = jnp.dot(p, ones_s[b * REACH : (b + 3) * REACH, :], preferred_element_type=f32)
        acc = jnp.where(lanes_of(acc.shape) == 0, top, acc)
        win_ref[:, b * REACH : (b + 1) * REACH, :] = acc.reshape(heads, REACH, LANES)


def attend_kernel(q_ref, win_ref, ctx_ref, sink_ref, bias_ref, _, out_ref, ones_s, done, sems):
    heads, n, _ = q_ref.shape
    copies = []
    kv = ctx_ref[...]
    ones_s[...] = with_ones(kv)
    step = REACH
    rows = heads * step
    lane = lanes_of((step, LANES))
    head = lax.broadcasted_iota(jnp.int32, (rows, 1), 0) // step
    bias, sink = jnp.zeros((rows, 1), f32), jnp.zeros((rows, 1), f32)
    for h in range(heads):
        bias = jnp.where(head == h, bias_ref[h], bias)
        sink = jnp.where(head == h, sink_ref[h], sink)
    for b in range(n // step):
        at = slice(b * step, (b + 1) * step)
        s = dot_nt(q_ref[:, at, :].reshape(rows, LANES), kv)
        win = win_ref[:, at, :].reshape(rows, LANES)
        win_top = win[:, 0:1]
        top = jnp.maximum(jnp.max(s, axis=1, keepdims=True) + bias, jnp.maximum(win_top, sink))
        p = jnp.exp(s - (top - bias)).astype(bf16)
        acc = jnp.dot(p, ones_s[...], preferred_element_type=f32)
        acc = acc + win * jnp.exp(win_top - top)
        den = acc[:, 1:2] + jnp.exp(sink - top)
        acc = (acc / den).reshape(heads, step, LANES)
        for pair in range(heads // 2):
            even = pltpu.roll(acc[2 * pair], HEAD, 1)
            both = jnp.where(lane < HEAD, even, acc[2 * pair + 1])
            done[at, pair * LANES : (pair + 1) * LANES] = both.astype(bf16)
        for k in range(out_ref.shape[0]):
            copy = pltpu.make_async_copy(done.at[at], out_ref.at[k, at], sems.at[b, k])
            copy.start()
            copies.append(copy)
    for copy in copies:
        copy.wait()


def out_kernel(att_ref, w_ref, x_ref, rows_ref, out_ref):
    sources, n, width = att_ref.shape
    t = lax.axis_index("tp")
    mixed = jnp.dot(att_ref[0], w_ref[0:width, :], preferred_element_type=f32)
    for k in range(1, sources):
        mixed = mixed + jnp.dot(
            att_ref[k], w_ref[k * width : (k + 1) * width, :], preferred_element_type=f32
        )
    low = lanes_of((1, LANES)) < 64
    for m in range(out_ref.shape[1] // LANES):
        cols = slice(m * LANES, (m + 1) * LANES)
        a = rows_ref[t * 8 + 2 * m, 2:3, :]
        b = rows_ref[t * 8 + 2 * m + 1, 2:3, :]
        gate = jnp.where(low, a, pltpu.roll(b, 64, 1))
        out_ref[:, cols] = x_ref[:, cols].astype(f32) + gate * mixed[:, cols]


def rotary_tables(rows, start):
    lane = np.arange(LANES)
    freq = ROTARY_BASE ** (-np.arange(0, 32, 2, dtype=np.float32) / 32)
    freq = jnp.asarray(freq[lane % 16].astype(np.float32))
    by_row = jnp.asarray(lane % 64 < 32)
    sign = jnp.asarray(np.where(lane % 32 < 16, -1.0, 1.0).astype(np.float32))
    position = start + jnp.arange(rows, dtype=jnp.int32)
    row, col = position // GRID_W, position % GRID_W
    place = jnp.where(by_row[None, :], row[:, None], col[:, None]).astype(f32)
    angle = place * freq[None, :]
    return jnp.cos(angle), jnp.sin(angle) * sign[None, :]


def per_device(
    latent, conditioning, context_cond, modulation, context, query_weight, key_projection,
    value_projection, out_weight, sink_head_logit, prefix_logit_bias,
):
    sp, tp = lax.axis_size("sp"), lax.axis_size("tp")
    spread = tp * lax.axis_size("dp")
    x, ctx = latent[0], context[0]
    n = x.shape[0]
    partial = call(
        partial_kernel,
        jax.ShapeDtypeStruct((sp, 16, LANES), bf16),
        [VMEM] * 3,
        [pltpu.VMEM((16, LANES), f32), pltpu.VMEM((16, LANES), f32)],
        56,
    )(conditioning, context_cond[None, :], modulation.transpose(0, 2, 1))
    with jax.named_scope("sums"):
        partials = lax.all_to_all(partial, "sp", 0, 0, tiled=True)
    flat = jax.ShapeDtypeStruct((n, LANES), f32)
    cflat = jax.ShapeDtypeStruct((ctx.shape[0], LANES), f32)
    mean, rstd, cmean, crstd = call(stats_kernel, (flat, flat, cflat, cflat), [VMEM] * 2, (), 8)(
        in_hbm(x), in_hbm(ctx)
    )
    wkv = jnp.concatenate([key_projection.T, value_projection.T], axis=0)
    cos, sin = rotary_tables(n, lax.axis_index("sp") * n)
    cols = out_weight.shape[1]
    own = lax.dynamic_slice_in_dim(x, lax.axis_index("tp") * cols, cols, 1)
    send = call(
        rows_kernel,
        jax.ShapeDtypeStruct((spread, 4, LANES), f32),
        [VMEM] + [ANY] * 5,
        [pltpu.VMEM((16, LANES), f32)],
        2,
    )(partials, cmean, wkv, cos, sin, own)
    with jax.named_scope("spread"):
        rows = lax.all_to_all(send, ("tp", "dp"), 0, 0, tiled=True)
    ctx_kv = call(
        ctx_kernel,
        jax.ShapeDtypeStruct((sp, ctx.shape[0], LANES), bf16),
        [VMEM] * 5,
        [pltpu.VMEM(ctx.shape, bf16)],
        4,
    )(ctx, cmean, crstd, rows, wkv)
    with jax.named_scope("context"):
        ctx_all = lax.all_to_all(ctx_kv, "sp", 0, 0, tiled=True).reshape(-1, LANES)
    heads = query_weight.shape[1] // HEAD
    edge = jax.ShapeDtypeStruct((REACH, LANES), bf16)
    q, kv, first, last = call(
        project_kernel,
        (
            jax.ShapeDtypeStruct((heads, n, LANES), bf16),
            jax.ShapeDtypeStruct((n, LANES), bf16),
            edge,
            edge,
        ),
        [VMEM] * 8,
        [pltpu.VMEM(x.shape, bf16)],
        6,
    )(in_hbm(x), mean, rstd, rows, in_hbm(query_weight), wkv, cos, sin)
    up = [(i, i + 1) for i in range(sp - 1)]
    down = [(i + 1, i) for i in range(sp - 1)]
    with jax.named_scope("halo"):
        before = lax.ppermute(last, "sp", up)
        after = lax.ppermute(first, "sp", down)
    wide = pltpu.VMEM((n + 2 * REACH, LANES), bf16)
    win = call(
        window_kernel,
        jax.ShapeDtypeStruct((heads, n, LANES), f32),
        [VMEM] * 4,
        [wide, wide],
        5,
    )(q, kv, before, after)
    attended = call(
        attend_kernel,
        pltpu.HBM((tp, n, heads * HEAD), bf16),
        [VMEM] * 3 + [SMEM] * 2 + [ANY],
        [
            pltpu.VMEM(ctx_all.shape, bf16),
            pltpu.VMEM((n, heads * HEAD), bf16),
            pltpu.SemaphoreType.DMA((n // REACH, tp)),
        ],
        8,
        ANY,
    )(q, win, ctx_all, sink_head_logit, prefix_logit_bias, out_weight)
    with jax.named_scope("heads"):
        every = lax.all_to_all(attended, "tp", 0, 0, tiled=True)
    out = call(out_kernel, jax.ShapeDtypeStruct((n, cols), f32), [VMEM] * 4, (), 8)(
        every, out_weight, own, rows
    )
    return out[None]


def solution(mesh):
    placed = (
        P("dp", "sp", None),
        P(None, "sp"),
        P("sp"),
        P(None, "sp", ("tp", "dp")),
        P("dp", "sp", None),
        P(None, "tp"),
        P(None, "tp"),
        P(None, "tp"),
        P(None, "tp"),
        P("tp"),
        P("tp"),
    )
    return jax.shard_map(
        per_device, mesh=mesh, in_specs=placed, out_specs=P("dp", "sp", "tp"), check_vma=False
    )
```

```python
import functools

import jax
import jax.numpy as jnp
import numpy as np
from jax import lax
from jax.experimental import pallas as pl
from jax.experimental.pallas import tpu as pltpu
from jax.sharding import PartitionSpec as P

HEAD = 64
GRID_W = 64
REACH = 128
EPS = 1e-06
ROTARY_BASE = 10000.0
MASKED = -1e30
LANES = 128
PARTIAL_ROWS = 24
GATE_ROWS = (9, 10, 11, 21)

f32 = jnp.float32
bf16 = jnp.bfloat16
VMEM = pl.BlockSpec(memory_space=pltpu.VMEM)
SMEM = pl.BlockSpec(memory_space=pltpu.SMEM)
ANY = pl.BlockSpec(memory_space=pl.ANY)


def in_hbm(x):
    return pltpu.with_memory_space_constraint(x, pltpu.HBM)


def dot_nt(a, b):
    return lax.dot_general(a, b, (((1,), (1,)), ((), ())), preferred_element_type=f32)


def lanes_of(shape):
    return lax.broadcasted_iota(jnp.int32, shape, len(shape) - 1)


def call(kernel, out_shape, ins, scratch=(), mib=8, out=VMEM):
    return pl.pallas_call(
        kernel,
        out_shape=out_shape,
        in_specs=ins,
        out_specs=jax.tree.map(lambda _: out, out_shape),
        scratch_shapes=list(scratch),
        compiler_params=pltpu.CompilerParams(vmem_limit_bytes=mib << 20),
    )


def partial_kernel(cond_ref, ctx_ref, mod_ref, out_ref, rows, packed):
    samples = cond_ref.shape[0]
    rows[...] = jnp.zeros_like(rows)
    rows[0:samples, :] = cond_ref[...].astype(f32)
    rows[samples : samples + 1, :] = ctx_ref[...].astype(f32)
    v = rows[...]
    act = (v / (1.0 + jnp.exp(-v))).astype(bf16)
    shift = dot_nt(act, mod_ref[0])
    scale = dot_nt(act, mod_ref[1])
    gate = dot_nt(act, mod_ref[2])
    both = jnp.concatenate([shift, scale], axis=1)
    gates = jnp.concatenate([gate[0:4], gate[4:8]], axis=1)
    packed[...] = jnp.zeros_like(packed)
    packed[0:9, :] = both[0:9]
    packed[12:21, :] = (both - both.astype(bf16).astype(f32))[0:9]
    for j, row in enumerate(GATE_ROWS):
        packed[row : row + 1, :] = gates[j : j + 1]
    out_ref[...] = jnp.broadcast_to(packed[...].astype(bf16)[None], out_ref.shape)


def rows_kernel(in_ref, *refs):
    out_ref, total = refs[-2:]
    total[...] = jnp.sum(in_ref[...].astype(f32), axis=0)
    total[0:9, :] = total[0:9, :] + total[12:21, :]
    copies = out_ref.shape[0] // 8
    for d in range(8):
        row = GATE_ROWS[d % 4]
        gate = total[row : row + 1, :]
        if d >= 4:
            gate = pltpu.roll(gate, 64, 1)
        for t in range(copies):
            out_ref[t * 8 + d, 0:1, :] = total[d : d + 1, :]
            out_ref[t * 8 + d, 1:2, :] = total[8:9, :]
            out_ref[t * 8 + d, 2:3, :] = gate
            out_ref[t * 8 + d, 3:4, :] = gate


def stats_of(x_ref, mean_ref, rstd_ref):
    width = x_ref.shape[1]
    step = 64

    def body(i, carry):
        at = pl.ds(pl.multiple_of(i * step, step), step)
        x = x_ref[at, :].astype(f32)
        mean = jnp.sum(x, axis=1, keepdims=True) * (1.0 / width)
        d = x - mean
        var = jnp.sum(d * d, axis=1, keepdims=True) * (1.0 / width)
        mean_ref[at, :] = jnp.broadcast_to(mean, (step, LANES))
        rstd_ref[at, :] = jnp.broadcast_to(lax.rsqrt(var + EPS), (step, LANES))
        return carry

    lax.fori_loop(0, x_ref.shape[0] // step, body, 0)


def stats_kernel(x_ref, c_ref, mean_ref, rstd_ref, cmean_ref, crstd_ref):
    stats_of(x_ref, mean_ref, rstd_ref)
    stats_of(c_ref, cmean_ref, crstd_ref)


def mod_tile(rows_ref, row, m):
    a = rows_ref[2 * m, row : row + 1, :]
    b = rows_ref[2 * m + 1, row : row + 1, :]
    low = lanes_of((1, LANES)) < 64
    shift = jnp.where(low, a, pltpu.roll(b, 64, 1))
    scale = jnp.where(low, pltpu.roll(a, 64, 1), b)
    return shift, 1.0 + scale


def modulate(x_ref, mean_ref, rstd_ref, rows_ref, row, out_ref, start):
    n = x_ref.shape[0]
    for m in range(x_ref.shape[1] // LANES):
        shift, scale = mod_tile(rows_ref, row, m)
        cols = slice(m * LANES, (m + 1) * LANES)
        x = x_ref[:, cols].astype(f32)
        y = (x - mean_ref[...]) * rstd_ref[...] * scale + shift
        out_ref[start : start + n, cols] = y.astype(bf16)


def ctx_kernel(x_ref, mean_ref, rstd_ref, rows_ref, wkv_ref, out_ref, normed):
    modulate(x_ref, mean_ref, rstd_ref, rows_ref, 1, normed, 0)
    kv = dot_nt(normed[...], wkv_ref[...]).astype(bf16)
    out_ref[...] = jnp.broadcast_to(kv[None], out_ref.shape)


def turned(u, cos, sin):
    low = lanes_of(u.shape) % 32 < 16
    other = jnp.where(low, pltpu.roll(u, LANES - 16, 1), pltpu.roll(u, 16, 1))
    return u * cos + other * sin


def with_ones(kv):
    return jnp.where(lanes_of(kv.shape) < HEAD, jnp.ones_like(kv), kv)


def project_kernel(
    x_ref, mean_ref, rstd_ref, rows_ref, wq_ref, wkv_ref, cos_ref, sin_ref,
    q_ref, kv_ref, head_ref, tail_ref, normed,
):
    n = x_ref.shape[0]
    modulate(x_ref, mean_ref, rstd_ref, rows_ref, 0, normed, 0)
    cos, sin = cos_ref[...], sin_ref[...]
    low = lanes_of((n, LANES)) < HEAD
    kv = dot_nt(normed[...], wkv_ref[...])
    kv = turned(kv, jnp.where(low, cos, 1.0), jnp.where(low, sin, 0.0)).astype(bf16)
    kv_ref[...] = kv
    head_ref[...] = kv[0:REACH]
    tail_ref[...] = kv[n - REACH : n]
    q = jnp.dot(normed[...], wq_ref[...], preferred_element_type=f32)
    for pair in range(q.shape[1] // LANES):
        u = turned(q[:, pair * LANES : (pair + 1) * LANES], cos, sin) * (HEAD ** -0.5)
        q_ref[2 * pair] = jnp.where(low, u, 0.0).astype(bf16)
        q_ref[2 * pair + 1] = jnp.where(low, pltpu.roll(u, HEAD, 1), 0.0).astype(bf16)


def window_kernel(q_ref, kv_ref, before_ref, after_ref, win_ref, kv_s, ones_s):
    heads, n, _ = q_ref.shape
    kv_s[0:REACH, :] = before_ref[...]
    kv_s[REACH : REACH + n, :] = kv_ref[...]
    kv_s[REACH + n :, :] = after_ref[...]
    ones_s[...] = with_ones(kv_s[...])
    rows = heads * REACH
    blocks = n // REACH
    i = lax.broadcasted_iota(jnp.int32, (rows, 3 * REACH), 0) % REACH
    j = lanes_of((rows, 3 * REACH))
    near = (j >= i) & (j <= i + 2 * REACH)
    place = lax.axis_index("sp")
    first, last = place == 0, place == lax.axis_size("sp") - 1
    for b in range(blocks):
        qb = q_ref[:, b * REACH : (b + 1) * REACH, :].reshape(rows, LANES)
        s = dot_nt(qb, kv_s[b * REACH : (b + 3) * REACH, :])
        valid = near
        if b == 0:
            valid = valid & (j >= jnp.where(first, REACH, 0))
        if b == blocks - 1:
            valid = valid & (j < jnp.where(last, 2 * REACH, 3 * REACH))
        s = jnp.where(valid, s, MASKED)
        top = jnp.max(s, axis=1, keepdims=True)
        p = jnp.exp(s - top).astype(bf16)
        acc = jnp.dot(p, ones_s[b * REACH : (b + 3) * REACH, :], preferred_element_type=f32)
        acc = jnp.where(lanes_of(acc.shape) == 0, top, acc)
        win_ref[:, b * REACH : (b + 1) * REACH, :] = acc.reshape(heads, REACH, LANES)


def attend_kernel(q_ref, win_ref, ctx_ref, sink_ref, bias_ref, _, out_ref, ones_s):
    heads, n, _ = q_ref.shape
    kv = ctx_ref[...]
    ones_s[...] = with_ones(kv)
    rows = heads * REACH
    lane = lanes_of((REACH, LANES))
    head = lax.broadcasted_iota(jnp.int32, (rows, 1), 0) // REACH
    bias, sink = jnp.zeros((rows, 1), f32), jnp.zeros((rows, 1), f32)
    for h in range(heads):
        bias = jnp.where(head == h, bias_ref[h], bias)
        sink = jnp.where(head == h, sink_ref[h], sink)
    for b in range(n // REACH):
        at = slice(b * REACH, (b + 1) * REACH)
        s = dot_nt(q_ref[:, at, :].reshape(rows, LANES), kv)
        win = win_ref[:, at, :].reshape(rows, LANES)
        win_top = win[:, 0:1]
        top = jnp.maximum(jnp.max(s, axis=1, keepdims=True) + bias, jnp.maximum(win_top, sink))
        p = jnp.exp(s - (top - bias)).astype(bf16)
        acc = jnp.dot(p, ones_s[...], preferred_element_type=f32)
        acc = acc + win * jnp.exp(win_top - top)
        den = acc[:, 1:2] + jnp.exp(sink - top)
        acc = (acc / den).reshape(heads, REACH, LANES)
        for pair in range(heads // 2):
            even = pltpu.roll(acc[2 * pair], HEAD, 1)
            both = jnp.where(lane < HEAD, even, acc[2 * pair + 1]).astype(bf16)
            for k in range(out_ref.shape[0]):
                out_ref[k, at, pair * LANES : (pair + 1) * LANES] = both


def out_kernel(att_ref, w_ref, x_ref, rows_ref, out_ref):
    sources, n, width = att_ref.shape
    t = lax.axis_index("tp")
    mixed = jnp.dot(att_ref[0], w_ref[0:width, :], preferred_element_type=f32)
    for k in range(1, sources):
        mixed = mixed + jnp.dot(
            att_ref[k], w_ref[k * width : (k + 1) * width, :], preferred_element_type=f32
        )
    low = lanes_of((1, LANES)) < 64
    for m in range(out_ref.shape[1] // LANES):
        cols = slice(m * LANES, (m + 1) * LANES)
        a = rows_ref[t * 8 + 2 * m, 2:3, :]
        b = rows_ref[t * 8 + 2 * m + 1, 2:3, :]
        gate = jnp.where(low, a, pltpu.roll(b, 64, 1))
        out_ref[:, cols] = x_ref[:, cols].astype(f32) + gate * mixed[:, cols]


def rotary_tables(rows, start):
    lane = np.arange(LANES)
    freq = ROTARY_BASE ** (-np.arange(0, 32, 2, dtype=np.float32) / 32)
    freq = jnp.asarray(freq[lane % 16].astype(np.float32))
    by_row = jnp.asarray(lane % 64 < 32)
    sign = jnp.asarray(np.where(lane % 32 < 16, -1.0, 1.0).astype(np.float32))
    position = start + jnp.arange(rows, dtype=jnp.int32)
    row, col = position // GRID_W, position % GRID_W
    place = jnp.where(by_row[None, :], row[:, None], col[:, None]).astype(f32)
    angle = place * freq[None, :]
    return jnp.cos(angle), jnp.sin(angle) * sign[None, :]


def per_device(
    latent, conditioning, context_cond, modulation, context, query_weight, key_projection,
    value_projection, out_weight, sink_head_logit, prefix_logit_bias,
):
    sp, tp = lax.axis_size("sp"), lax.axis_size("tp")
    spread = tp * lax.axis_size("dp")
    x, ctx = latent[0], context[0]
    n = x.shape[0]
    partial = call(
        partial_kernel,
        jax.ShapeDtypeStruct((sp, PARTIAL_ROWS, LANES), bf16),
        [VMEM] * 3,
        [pltpu.VMEM((16, LANES), f32), pltpu.VMEM((PARTIAL_ROWS, LANES), f32)],
        56,
    )(conditioning, context_cond[None, :], modulation.transpose(0, 2, 1))
    with jax.named_scope("sums"):
        partials = lax.all_to_all(partial, "sp", 0, 0, tiled=True)
    flat = jax.ShapeDtypeStruct((n, LANES), f32)
    cflat = jax.ShapeDtypeStruct((ctx.shape[0], LANES), f32)
    mean, rstd, cmean, crstd = call(stats_kernel, (flat, flat, cflat, cflat), [VMEM] * 2, (), 8)(
        in_hbm(x), in_hbm(ctx)
    )
    wkv = jnp.concatenate([key_projection.T, value_projection.T], axis=0)
    cos, sin = rotary_tables(n, lax.axis_index("sp") * n)
    cols = out_weight.shape[1]
    own = lax.dynamic_slice_in_dim(x, lax.axis_index("tp") * cols, cols, 1)
    send = call(
        rows_kernel,
        jax.ShapeDtypeStruct((spread, 4, LANES), f32),
        [VMEM] + [ANY] * 5,
        [pltpu.VMEM((PARTIAL_ROWS, LANES), f32)],
        2,
    )(partials, cmean, wkv, cos, sin, own)
    with jax.named_scope("spread"):
        rows = lax.all_to_all(send, ("tp", "dp"), 0, 0, tiled=True)
    ctx_kv = call(
        ctx_kernel,
        jax.ShapeDtypeStruct((sp, ctx.shape[0], LANES), bf16),
        [VMEM] * 5,
        [pltpu.VMEM(ctx.shape, bf16)],
        4,
    )(ctx, cmean, crstd, rows, wkv)
    with jax.named_scope("context"):
        ctx_all = lax.all_to_all(ctx_kv, "sp", 0, 0, tiled=True).reshape(-1, LANES)
    heads = query_weight.shape[1] // HEAD
    edge = jax.ShapeDtypeStruct((REACH, LANES), bf16)
    q, kv, first, last = call(
        project_kernel,
        (
            jax.ShapeDtypeStruct((heads, n, LANES), bf16),
            jax.ShapeDtypeStruct((n, LANES), bf16),
            edge,
            edge,
        ),
        [VMEM] * 8,
        [pltpu.VMEM(x.shape, bf16)],
        6,
    )(in_hbm(x), mean, rstd, rows, in_hbm(query_weight), wkv, cos, sin)
    up = [(i, i + 1) for i in range(sp - 1)]
    down = [(i + 1, i) for i in range(sp - 1)]
    with jax.named_scope("halo"):
        before = lax.ppermute(last, "sp", up)
        after = lax.ppermute(first, "sp", down)
    wide = pltpu.VMEM((n + 2 * REACH, LANES), bf16)
    win = call(
        window_kernel,
        jax.ShapeDtypeStruct((heads, n, LANES), f32),
        [VMEM] * 4,
        [wide, wide],
        5,
    )(q, kv, before, after)
    attended = call(
        attend_kernel,
        jax.ShapeDtypeStruct((tp, n, heads * HEAD), bf16),
        [VMEM] * 3 + [SMEM] * 2 + [ANY],
        [pltpu.VMEM(ctx_all.shape, bf16)],
        8,
    )(q, win, ctx_all, sink_head_logit, prefix_logit_bias, out_weight)
    with jax.named_scope("heads"):
        every = lax.all_to_all(attended, "tp", 0, 0, tiled=True)
    out = call(out_kernel, jax.ShapeDtypeStruct((n, cols), f32), [VMEM] * 4, (), 8)(
        every, out_weight, own, rows
    )
    return out[None]


def solution(mesh):
    placed = (
        P("dp", "sp", None),
        P(None, "sp"),
        P("sp"),
        P(None, "sp", ("tp", "dp")),
        P("dp", "sp", None),
        P(None, "tp"),
        P(None, "tp"),
        P(None, "tp"),
        P(None, "tp"),
        P("tp"),
        P("tp"),
    )
    return jax.shard_map(
        per_device, mesh=mesh, in_specs=placed, out_specs=P("dp", "sp", "tp"), check_vma=False
    )
```

```python
import functools

import jax
import jax.numpy as jnp
import numpy as np
from jax import lax
from jax.experimental import pallas as pl
from jax.experimental.pallas import tpu as pltpu
from jax.sharding import PartitionSpec as P

HEAD = 64
GRID_W = 64
REACH = 128
EPS = 1e-06
ROTARY_BASE = 10000.0
MASKED = -1e30
LANES = 128
PARTIAL_ROWS = 24
GATE_ROWS = (9, 10, 11, 21)

f32 = jnp.float32
bf16 = jnp.bfloat16
VMEM = pl.BlockSpec(memory_space=pltpu.VMEM)
SMEM = pl.BlockSpec(memory_space=pltpu.SMEM)
ANY = pl.BlockSpec(memory_space=pl.ANY)


def in_hbm(x):
    return pltpu.with_memory_space_constraint(x, pltpu.HBM)


def dot_nt(a, b):
    return lax.dot_general(a, b, (((1,), (1,)), ((), ())), preferred_element_type=f32)


def lanes_of(shape):
    return lax.broadcasted_iota(jnp.int32, shape, len(shape) - 1)


def call(kernel, out_shape, ins, scratch=(), mib=8, out=VMEM):
    return pl.pallas_call(
        kernel,
        out_shape=out_shape,
        in_specs=ins,
        out_specs=jax.tree.map(lambda _: out, out_shape),
        scratch_shapes=list(scratch),
        compiler_params=pltpu.CompilerParams(vmem_limit_bytes=mib << 20),
    )


def partial_kernel(cond_ref, ctx_ref, mod_ref, out_ref, rows, packed):
    samples = cond_ref.shape[0]
    rows[...] = jnp.zeros_like(rows)
    rows[0:samples, :] = cond_ref[...].astype(f32)
    rows[samples : samples + 1, :] = ctx_ref[...].astype(f32)
    v = rows[...]
    act = (v / (1.0 + jnp.exp(-v))).astype(bf16)
    shift = dot_nt(act, mod_ref[0])
    scale = dot_nt(act, mod_ref[1])
    gate = dot_nt(act, mod_ref[2])
    both = jnp.concatenate([shift, scale], axis=1)
    gates = jnp.concatenate([gate[0:4], gate[4:8]], axis=1)
    packed[...] = jnp.zeros_like(packed)
    packed[0:9, :] = both[0:9]
    packed[12:21, :] = (both - both.astype(bf16).astype(f32))[0:9]
    for j, row in enumerate(GATE_ROWS):
        packed[row : row + 1, :] = gates[j : j + 1]
    out_ref[...] = jnp.broadcast_to(packed[...].astype(bf16)[None], out_ref.shape)


def rows_kernel(in_ref, *refs):
    out_ref, total = refs[-2:]
    total[...] = jnp.sum(in_ref[...].astype(f32), axis=0)
    total[0:9, :] = total[0:9, :] + total[12:21, :]
    copies = out_ref.shape[0] // 8
    for d in range(8):
        row = GATE_ROWS[d % 4]
        gate = total[row : row + 1, :]
        if d >= 4:
            gate = pltpu.roll(gate, 64, 1)
        for t in range(copies):
            out_ref[t * 8 + d, 0:1, :] = total[d : d + 1, :]
            out_ref[t * 8 + d, 1:2, :] = total[8:9, :]
            out_ref[t * 8 + d, 2:3, :] = gate
            out_ref[t * 8 + d, 3:4, :] = gate


def stats_of(x_ref, mean_ref, rstd_ref):
    width = x_ref.shape[1]
    step = 64

    def body(i, carry):
        at = pl.ds(pl.multiple_of(i * step, step), step)
        x = x_ref[at, :].astype(f32)
        mean = jnp.sum(x, axis=1, keepdims=True) * (1.0 / width)
        d = x - mean
        var = jnp.sum(d * d, axis=1, keepdims=True) * (1.0 / width)
        mean_ref[at, :] = jnp.broadcast_to(mean, (step, LANES))
        rstd_ref[at, :] = jnp.broadcast_to(lax.rsqrt(var + EPS), (step, LANES))
        return carry

    lax.fori_loop(0, x_ref.shape[0] // step, body, 0)


def stats_kernel(x_ref, c_ref, mean_ref, rstd_ref, cmean_ref, crstd_ref):
    stats_of(x_ref, mean_ref, rstd_ref)
    stats_of(c_ref, cmean_ref, crstd_ref)


def mod_tile(rows_ref, row, m):
    a = rows_ref[2 * m, row : row + 1, :]
    b = rows_ref[2 * m + 1, row : row + 1, :]
    low = lanes_of((1, LANES)) < 64
    shift = jnp.where(low, a, pltpu.roll(b, 64, 1))
    scale = jnp.where(low, pltpu.roll(a, 64, 1), b)
    return shift, 1.0 + scale


def modulate(x_ref, mean_ref, rstd_ref, rows_ref, row, out_ref, start):
    n = x_ref.shape[0]
    for m in range(x_ref.shape[1] // LANES):
        shift, scale = mod_tile(rows_ref, row, m)
        cols = slice(m * LANES, (m + 1) * LANES)
        x = x_ref[:, cols].astype(f32)
        y = (x - mean_ref[...]) * rstd_ref[...] * scale + shift
        out_ref[start : start + n, cols] = y.astype(bf16)


def ctx_kernel(x_ref, mean_ref, rstd_ref, rows_ref, wkv_ref, out_ref):
    acc = jnp.zeros((x_ref.shape[0], LANES), f32)
    for m in range(0, x_ref.shape[1] // LANES, 2):
        parts = []
        for k in (m, m + 1):
            shift, scale = mod_tile(rows_ref, 1, k)
            x = x_ref[:, k * LANES : (k + 1) * LANES].astype(f32)
            y = (x - mean_ref[...]) * rstd_ref[...] * scale + shift
            parts.append(y.astype(bf16))
        wide = slice(m * LANES, (m + 2) * LANES)
        acc = acc + dot_nt(jnp.concatenate(parts, axis=1), wkv_ref[:, wide])
    out_ref[...] = jnp.broadcast_to(acc.astype(bf16)[None], out_ref.shape)


def turned(u, cos, sin):
    low = lanes_of(u.shape) % 32 < 16
    other = jnp.where(low, pltpu.roll(u, LANES - 16, 1), pltpu.roll(u, 16, 1))
    return u * cos + other * sin


def with_ones(kv):
    return jnp.where(lanes_of(kv.shape) < HEAD, jnp.ones_like(kv), kv)


def project_kernel(
    x_ref, mean_ref, rstd_ref, rows_ref, wq_ref, wkv_ref, row_ref, col_ref,
    q_ref, kv_ref, head_ref, tail_ref, normed, cos_s, sin_s,
):
    n = x_ref.shape[0]
    modulate(x_ref, mean_ref, rstd_ref, rows_ref, 0, normed, 0)
    by_row = lanes_of((GRID_W, LANES)) % HEAD < HEAD // 2
    first = lax.axis_index("sp") * (n // GRID_W)
    for g in range(n // GRID_W):
        at = slice(g * GRID_W, (g + 1) * GRID_W)
        cos_s[at, :] = jnp.where(by_row, row_ref[0, pl.ds(first + g, 1), :], col_ref[0])
        sin_s[at, :] = jnp.where(by_row, row_ref[1, pl.ds(first + g, 1), :], col_ref[1])
    cos, sin = cos_s[...], sin_s[...]
    low = lanes_of((n, LANES)) < HEAD
    kv = dot_nt(normed[...], wkv_ref[...])
    kv = turned(kv, jnp.where(low, cos, 1.0), jnp.where(low, sin, 0.0)).astype(bf16)
    kv_ref[...] = kv
    head_ref[...] = kv[0:REACH]
    tail_ref[...] = kv[n - REACH : n]
    q = jnp.dot(normed[...], wq_ref[...], preferred_element_type=f32)
    for pair in range(q.shape[1] // LANES):
        u = turned(q[:, pair * LANES : (pair + 1) * LANES], cos, sin) * (HEAD ** -0.5)
        q_ref[2 * pair] = jnp.where(low, u, 0.0).astype(bf16)
        q_ref[2 * pair + 1] = jnp.where(low, pltpu.roll(u, HEAD, 1), 0.0).astype(bf16)


def window_kernel(q_ref, kv_ref, before_ref, after_ref, win_ref, kv_s, ones_s):
    heads, n, _ = q_ref.shape
    kv_s[0:REACH, :] = before_ref[...]
    kv_s[REACH : REACH + n, :] = kv_ref[...]
    kv_s[REACH + n :, :] = after_ref[...]
    ones_s[...] = with_ones(kv_s[...])
    rows = heads * REACH
    blocks = n // REACH
    i = lax.broadcasted_iota(jnp.int32, (rows, 3 * REACH), 0) % REACH
    j = lanes_of((rows, 3 * REACH))
    near = (j >= i) & (j <= i + 2 * REACH)
    place = lax.axis_index("sp")
    first, last = place == 0, place == lax.axis_size("sp") - 1
    for b in range(blocks):
        qb = q_ref[:, b * REACH : (b + 1) * REACH, :].reshape(rows, LANES)
        s = dot_nt(qb, kv_s[b * REACH : (b + 3) * REACH, :])
        valid = near
        if b == 0:
            valid = valid & (j >= jnp.where(first, REACH, 0))
        if b == blocks - 1:
            valid = valid & (j < jnp.where(last, 2 * REACH, 3 * REACH))
        s = jnp.where(valid, s, MASKED)
        top = jnp.max(s, axis=1, keepdims=True)
        p = jnp.exp(s - top).astype(bf16)
        acc = jnp.dot(p, ones_s[b * REACH : (b + 3) * REACH, :], preferred_element_type=f32)
        acc = jnp.where(lanes_of(acc.shape) == 0, top, acc)
        win_ref[:, b * REACH : (b + 1) * REACH, :] = acc.reshape(heads, REACH, LANES)


def attend_kernel(q_ref, win_ref, ctx_ref, sink_ref, bias_ref, _, out_ref, ones_s):
    heads, n, _ = q_ref.shape
    kv = ctx_ref[...]
    ones_s[...] = with_ones(kv)
    rows = heads * REACH
    lane = lanes_of((REACH, LANES))
    head = lax.broadcasted_iota(jnp.int32, (rows, 1), 0) // REACH
    bias, sink = jnp.zeros((rows, 1), f32), jnp.zeros((rows, 1), f32)
    for h in range(heads):
        bias = jnp.where(head == h, bias_ref[h], bias)
        sink = jnp.where(head == h, sink_ref[h], sink)
    for b in range(n // REACH):
        at = slice(b * REACH, (b + 1) * REACH)
        s = dot_nt(q_ref[:, at, :].reshape(rows, LANES), kv)
        win = win_ref[:, at, :].reshape(rows, LANES)
        win_top = win[:, 0:1]
        top = jnp.maximum(jnp.max(s, axis=1, keepdims=True) + bias, jnp.maximum(win_top, sink))
        p = jnp.exp(s - (top - bias)).astype(bf16)
        acc = jnp.dot(p, ones_s[...], preferred_element_type=f32)
        acc = acc + win * jnp.exp(win_top - top)
        den = acc[:, 1:2] + jnp.exp(sink - top)
        acc = (acc / den).reshape(heads, REACH, LANES)
        for pair in range(heads // 2):
            even = pltpu.roll(acc[2 * pair], HEAD, 1)
            both = jnp.where(lane < HEAD, even, acc[2 * pair + 1]).astype(bf16)
            for k in range(out_ref.shape[0]):
                out_ref[k, at, pair * LANES : (pair + 1) * LANES] = both


def out_kernel(att_ref, w_ref, x_ref, rows_ref, out_ref, ready, sems):
    sources, n, _ = att_ref.shape
    t = lax.axis_index("tp")
    low = lanes_of((1, LANES)) < 64
    copies = []
    for i in range(n // REACH):
        at = slice(i * REACH, (i + 1) * REACH)
        att = jnp.concatenate([att_ref[k, at, :] for k in range(sources)], axis=1)
        mixed = jnp.dot(att, w_ref[...], preferred_element_type=f32)
        for m in range(out_ref.shape[1] // LANES):
            cols = slice(m * LANES, (m + 1) * LANES)
            a = rows_ref[t * 8 + 2 * m, 2:3, :]
            b = rows_ref[t * 8 + 2 * m + 1, 2:3, :]
            gate = jnp.where(low, a, pltpu.roll(b, 64, 1))
            ready[at, cols] = x_ref[at, cols].astype(f32) + gate * mixed[:, cols]
        copy = pltpu.make_async_copy(ready.at[at], out_ref.at[at], sems.at[i])
        copy.start()
        copies.append(copy)
    for copy in copies:
        copy.wait()


def rotary_table(places):
    lane = np.arange(LANES)
    freq = (ROTARY_BASE ** (-np.arange(0, 32, 2, dtype=np.float32) / 32)).astype(np.float32)
    angle = np.arange(places, dtype=np.float32)[:, None] * freq[lane % 16][None, :]
    sign = np.where(lane % 32 < 16, -1.0, 1.0)
    return np.stack([np.cos(angle), np.sin(angle) * sign[None, :]]).astype(np.float32)


def per_device(
    latent, conditioning, context_cond, modulation, context, query_weight, key_projection,
    value_projection, out_weight, sink_head_logit, prefix_logit_bias,
):
    sp, tp = lax.axis_size("sp"), lax.axis_size("tp")
    spread = tp * lax.axis_size("dp")
    x, ctx = latent[0], context[0]
    n = x.shape[0]
    partial = call(
        partial_kernel,
        jax.ShapeDtypeStruct((sp, PARTIAL_ROWS, LANES), bf16),
        [VMEM] * 3,
        [pltpu.VMEM((16, LANES), f32), pltpu.VMEM((PARTIAL_ROWS, LANES), f32)],
        56,
    )(conditioning, context_cond[None, :], modulation.transpose(0, 2, 1))
    with jax.named_scope("sums"):
        partials = lax.all_to_all(partial, "sp", 0, 0, tiled=True)
    flat = jax.ShapeDtypeStruct((n, LANES), f32)
    cflat = jax.ShapeDtypeStruct((ctx.shape[0], LANES), f32)
    mean, rstd, cmean, crstd = call(stats_kernel, (flat, flat, cflat, cflat), [VMEM] * 2, (), 8)(
        in_hbm(x), in_hbm(ctx)
    )
    wkv = jnp.concatenate([key_projection.T, value_projection.T], axis=0)
    by_row = jnp.asarray(rotary_table(sp * n // GRID_W))
    by_col = jnp.asarray(rotary_table(GRID_W))
    cols = out_weight.shape[1]
    own = lax.dynamic_slice_in_dim(x, lax.axis_index("tp") * cols, cols, 1)
    send = call(
        rows_kernel,
        jax.ShapeDtypeStruct((spread, 4, LANES), f32),
        [VMEM] + [ANY] * 3,
        [pltpu.VMEM((PARTIAL_ROWS, LANES), f32)],
        2,
    )(partials, cmean, wkv, own)
    with jax.named_scope("spread"):
        rows = lax.all_to_all(send, ("tp", "dp"), 0, 0, tiled=True)
    ctx_kv = call(
        ctx_kernel,
        jax.ShapeDtypeStruct((sp, ctx.shape[0], LANES), bf16),
        [VMEM] * 5,
        [],
        4,
    )(ctx, cmean, crstd, rows, wkv)
    with jax.named_scope("context"):
        ctx_all = lax.all_to_all(ctx_kv, "sp", 0, 0, tiled=True).reshape(-1, LANES)
    heads = query_weight.shape[1] // HEAD
    edge = jax.ShapeDtypeStruct((REACH, LANES), bf16)
    q, kv, first, last = call(
        project_kernel,
        (
            jax.ShapeDtypeStruct((heads, n, LANES), bf16),
            jax.ShapeDtypeStruct((n, LANES), bf16),
            edge,
            edge,
        ),
        [VMEM] * 8,
        [
            pltpu.VMEM(x.shape, bf16),
            pltpu.VMEM((n, LANES), f32),
            pltpu.VMEM((n, LANES), f32),
        ],
        7,
    )(in_hbm(x), mean, rstd, rows, in_hbm(query_weight), wkv, by_row, by_col)
    up = [(i, i + 1) for i in range(sp - 1)]
    down = [(i + 1, i) for i in range(sp - 1)]
    with jax.named_scope("halo"):
        before = lax.ppermute(last, "sp", up)
        after = lax.ppermute(first, "sp", down)
    wide = pltpu.VMEM((n + 2 * REACH, LANES), bf16)
    win = call(
        window_kernel,
        jax.ShapeDtypeStruct((heads, n, LANES), f32),
        [VMEM] * 4,
        [wide, wide],
        5,
    )(q, kv, before, after)
    attended = call(
        attend_kernel,
        jax.ShapeDtypeStruct((tp, n, heads * HEAD), bf16),
        [VMEM] * 3 + [SMEM] * 2 + [ANY],
        [pltpu.VMEM(ctx_all.shape, bf16)],
        8,
    )(q, win, ctx_all, sink_head_logit, prefix_logit_bias, out_weight)
    with jax.named_scope("heads"):
        every = lax.all_to_all(attended, "tp", 0, 0, tiled=True)
    out = call(
        out_kernel,
        pltpu.HBM((n, cols), f32),
        [VMEM] * 4,
        [pltpu.VMEM((n, cols), f32), pltpu.SemaphoreType.DMA((n // REACH,))],
        8,
        ANY,
    )(every, out_weight, own, rows)
    return out[None]


def solution(mesh):
    placed = (
        P("dp", "sp", None),
        P(None, "sp"),
        P("sp"),
        P(None, "sp", ("tp", "dp")),
        P("dp", "sp", None),
        P(None, "tp"),
        P(None, "tp"),
        P(None, "tp"),
        P(None, "tp"),
        P("tp"),
        P("tp"),
    )
    return jax.shard_map(
        per_device, mesh=mesh, in_specs=placed, out_specs=P("dp", "sp", "tp"), check_vma=False
    )
```

```python
import functools

import jax
import jax.numpy as jnp
import numpy as np
from jax import lax
from jax.experimental import pallas as pl
from jax.experimental.pallas import tpu as pltpu
from jax.sharding import PartitionSpec as P

HEAD = 64
GRID_W = 64
REACH = 128
EPS = 1e-06
ROTARY_BASE = 10000.0
MASKED = -1e30
LANES = 128
PARTIAL_ROWS = 24
GATE_ROWS = (9, 10, 11, 21)

f32 = jnp.float32
bf16 = jnp.bfloat16
VMEM = pl.BlockSpec(memory_space=pltpu.VMEM)
SMEM = pl.BlockSpec(memory_space=pltpu.SMEM)
ANY = pl.BlockSpec(memory_space=pl.ANY)


def in_hbm(x):
    return pltpu.with_memory_space_constraint(x, pltpu.HBM)


def dot_nt(a, b):
    return lax.dot_general(a, b, (((1,), (1,)), ((), ())), preferred_element_type=f32)


def lanes_of(shape):
    return lax.broadcasted_iota(jnp.int32, shape, len(shape) - 1)


def call(kernel, out_shape, ins, scratch=(), mib=8, out=VMEM):
    return pl.pallas_call(
        kernel,
        out_shape=out_shape,
        in_specs=ins,
        out_specs=jax.tree.map(lambda _: out, out_shape),
        scratch_shapes=list(scratch),
        compiler_params=pltpu.CompilerParams(vmem_limit_bytes=mib << 20),
    )


def partial_kernel(cond_ref, ctx_ref, mod_ref, out_ref, rows, packed):
    samples = cond_ref.shape[0]
    rows[...] = jnp.zeros_like(rows)
    rows[0:samples, :] = cond_ref[...].astype(f32)
    rows[samples : samples + 1, :] = ctx_ref[...].astype(f32)
    v = rows[...]
    act = (v / (1.0 + jnp.exp(-v))).astype(bf16)
    shift = dot_nt(act, mod_ref[0])
    scale = dot_nt(act, mod_ref[1])
    gate = dot_nt(act, mod_ref[2])
    both = jnp.concatenate([shift, scale], axis=1)
    gates = jnp.concatenate([gate[0:4], gate[4:8]], axis=1)
    packed[...] = jnp.zeros_like(packed)
    packed[0:9, :] = both[0:9]
    packed[12:21, :] = (both - both.astype(bf16).astype(f32))[0:9]
    for j, row in enumerate(GATE_ROWS):
        packed[row : row + 1, :] = gates[j : j + 1]
    out_ref[...] = jnp.broadcast_to(packed[...].astype(bf16)[None], out_ref.shape)


def rows_kernel(in_ref, *refs):
    out_ref, total = refs[-2:]
    total[...] = jnp.sum(in_ref[...].astype(f32), axis=0)
    total[0:9, :] = total[0:9, :] + total[12:21, :]
    copies = out_ref.shape[0] // 8
    for d in range(8):
        row = GATE_ROWS[d % 4]
        gate = total[row : row + 1, :]
        if d >= 4:
            gate = pltpu.roll(gate, 64, 1)
        for t in range(copies):
            out_ref[t * 8 + d, 0:1, :] = total[d : d + 1, :]
            out_ref[t * 8 + d, 1:2, :] = total[8:9, :]
            out_ref[t * 8 + d, 2:3, :] = gate
            out_ref[t * 8 + d, 3:4, :] = gate


def stats_of(x_ref, mean_ref, rstd_ref):
    width = x_ref.shape[1]
    step = 64

    def body(i, carry):
        at = pl.ds(pl.multiple_of(i * step, step), step)
        x = x_ref[at, :].astype(f32)
        mean = jnp.sum(x, axis=1, keepdims=True) * (1.0 / width)
        d = x - mean
        var = jnp.sum(d * d, axis=1, keepdims=True) * (1.0 / width)
        mean_ref[at, :] = jnp.broadcast_to(mean, (step, LANES))
        rstd_ref[at, :] = jnp.broadcast_to(lax.rsqrt(var + EPS), (step, LANES))
        return carry

    lax.fori_loop(0, x_ref.shape[0] // step, body, 0)


def stats_kernel(x_ref, c_ref, mean_ref, rstd_ref, cmean_ref, crstd_ref):
    stats_of(x_ref, mean_ref, rstd_ref)
    stats_of(c_ref, cmean_ref, crstd_ref)


def mod_tile(rows_ref, row, m):
    a = rows_ref[2 * m, row : row + 1, :]
    b = rows_ref[2 * m + 1, row : row + 1, :]
    low = lanes_of((1, LANES)) < 64
    shift = jnp.where(low, a, pltpu.roll(b, 64, 1))
    scale = jnp.where(low, pltpu.roll(a, 64, 1), b)
    return shift, 1.0 + scale


def modulate(x_ref, mean_ref, rstd_ref, rows_ref, row, out_ref, start):
    n = x_ref.shape[0]
    for m in range(x_ref.shape[1] // LANES):
        shift, scale = mod_tile(rows_ref, row, m)
        cols = slice(m * LANES, (m + 1) * LANES)
        x = x_ref[:, cols].astype(f32)
        y = (x - mean_ref[...]) * rstd_ref[...] * scale + shift
        out_ref[start : start + n, cols] = y.astype(bf16)


def ctx_kernel(x_ref, mean_ref, rstd_ref, rows_ref, wkv_ref, out_ref):
    acc = jnp.zeros((x_ref.shape[0], LANES), f32)
    for m in range(0, x_ref.shape[1] // LANES, 2):
        parts = []
        for k in (m, m + 1):
            shift, scale = mod_tile(rows_ref, 1, k)
            x = x_ref[:, k * LANES : (k + 1) * LANES].astype(f32)
            y = (x - mean_ref[...]) * rstd_ref[...] * scale + shift
            parts.append(y.astype(bf16))
        wide = slice(m * LANES, (m + 2) * LANES)
        acc = acc + dot_nt(jnp.concatenate(parts, axis=1), wkv_ref[:, wide])
    out_ref[...] = jnp.broadcast_to(acc.astype(bf16)[None], out_ref.shape)


def turned(u, cos, sin):
    low = lanes_of(u.shape) % 32 < 16
    other = jnp.where(low, pltpu.roll(u, LANES - 16, 1), pltpu.roll(u, 16, 1))
    return u * cos + other * sin


def with_ones(kv):
    return jnp.where(lanes_of(kv.shape) < HEAD, jnp.ones_like(kv), kv)


def project_kernel(
    x_ref, mean_ref, rstd_ref, rows_ref, wq_ref, wkv_ref, row_ref, col_ref,
    q_ref, kv_ref, head_ref, tail_ref, normed, cos_s, sin_s,
):
    n = x_ref.shape[0]
    modulate(x_ref, mean_ref, rstd_ref, rows_ref, 0, normed, 0)
    by_row = lanes_of((GRID_W, LANES)) % HEAD < HEAD // 2
    first = lax.axis_index("sp") * (n // GRID_W)
    for g in range(n // GRID_W):
        at = slice(g * GRID_W, (g + 1) * GRID_W)
        cos_s[at, :] = jnp.where(by_row, row_ref[0, pl.ds(first + g, 1), :], col_ref[0])
        sin_s[at, :] = jnp.where(by_row, row_ref[1, pl.ds(first + g, 1), :], col_ref[1])
    cos, sin = cos_s[...], sin_s[...]
    low = lanes_of((n, LANES)) < HEAD
    kv = dot_nt(normed[...], wkv_ref[...])
    kv = turned(kv, jnp.where(low, cos, 1.0), jnp.where(low, sin, 0.0)).astype(bf16)
    kv_ref[...] = kv
    head_ref[...] = kv[0:REACH]
    tail_ref[...] = kv[n - REACH : n]
    q = jnp.dot(normed[...], wq_ref[...], preferred_element_type=f32)
    for pair in range(q.shape[1] // LANES):
        u = turned(q[:, pair * LANES : (pair + 1) * LANES], cos, sin) * (HEAD ** -0.5)
        q_ref[2 * pair] = jnp.where(low, u, 0.0).astype(bf16)
        q_ref[2 * pair + 1] = jnp.where(low, pltpu.roll(u, HEAD, 1), 0.0).astype(bf16)


def window_kernel(q_ref, kv_ref, before_ref, after_ref, win_ref, kv_s, ones_s):
    heads, n, _ = q_ref.shape
    kv_s[0:REACH, :] = before_ref[...]
    kv_s[REACH : REACH + n, :] = kv_ref[...]
    kv_s[REACH + n :, :] = after_ref[...]
    ones_s[...] = with_ones(kv_s[...])
    rows = heads * REACH
    blocks = n // REACH
    i = lax.broadcasted_iota(jnp.int32, (rows, 3 * REACH), 0) % REACH
    j = lanes_of((rows, 3 * REACH))
    near = (j >= i) & (j <= i + 2 * REACH)
    place = lax.axis_index("sp")
    first, last = place == 0, place == lax.axis_size("sp") - 1
    for b in range(blocks):
        qb = q_ref[:, b * REACH : (b + 1) * REACH, :].reshape(rows, LANES)
        s = dot_nt(qb, kv_s[b * REACH : (b + 3) * REACH, :])
        valid = near
        if b == 0:
            valid = valid & (j >= jnp.where(first, REACH, 0))
        if b == blocks - 1:
            valid = valid & (j < jnp.where(last, 2 * REACH, 3 * REACH))
        s = jnp.where(valid, s, MASKED)
        top = jnp.max(s, axis=1, keepdims=True)
        p = jnp.exp(s - top).astype(bf16)
        acc = jnp.dot(p, ones_s[b * REACH : (b + 3) * REACH, :], preferred_element_type=f32)
        acc = jnp.where(lanes_of(acc.shape) == 0, top, acc)
        win_ref[:, b * REACH : (b + 1) * REACH, :] = acc.reshape(heads, REACH, LANES)


def top_of(s):
    m = s[:, 0:LANES]
    for k in range(1, s.shape[1] // LANES):
        m = jnp.maximum(m, s[:, k * LANES : (k + 1) * LANES])
    return jnp.max(m, axis=1, keepdims=True)


def attend_kernel(q_ref, win_ref, ctx_ref, sink_ref, bias_ref, _, out_ref, ones_s):
    heads, n, _ = q_ref.shape
    kv = ctx_ref[...]
    ones_s[...] = with_ones(kv)
    lane = lanes_of((REACH, LANES))

    sub = 2
    rows = sub * REACH
    def part(x, fill):
        head = lax.broadcasted_iota(jnp.int32, (rows, 1), 0) // REACH
        out = jnp.zeros((rows, 1), f32)
        for h in range(sub):
            out = jnp.where(head == h, x[fill + h], out)
        return out
    units = [(b, g) for b in range(n // REACH) for g in range(heads // sub)]
    biases = [part(bias_ref, g * sub) for g in range(heads // sub)]
    sinks = [part(sink_ref, g * sub) for g in range(heads // sub)]
    def score(u):
        b, g = u
        at = slice(b * REACH, (b + 1) * REACH)
        q = q_ref[g * sub : (g + 1) * sub, at, :].reshape(rows, LANES)
        return dot_nt(q, ctx_ref[...])
    ahead = 2
    queue = [score(u) for u in units[:ahead]]
    done = []
    for i, (b, g) in enumerate(units):
        if ahead == 0:
            s = score((b, g))
        else:
            s = queue.pop(0)
            if i + ahead < len(units):
                queue.append(score(units[i + ahead]))
        at = slice(b * REACH, (b + 1) * REACH)
        win = win_ref[g * sub : (g + 1) * sub, at, :].reshape(rows, LANES)
        win_top = win[:, 0:1]
        bias, sink = biases[g], sinks[g]
        top = jnp.maximum(top_of(s) + bias, jnp.maximum(win_top, sink))
        p = jnp.exp(s - (top - bias)).astype(bf16)
        acc = jnp.dot(p, ones_s[...], preferred_element_type=f32) + win * jnp.exp(win_top - top)
        acc = (acc * (1.0 / (acc[:, 1:2] + jnp.exp(sink - top)))).reshape(sub, REACH, LANES)
        if g == 0:
            done = []
        done.extend(acc[h] for h in range(sub))
        if g < heads // sub - 1:
            continue

        for pair in range(heads // 2):
            even = pltpu.roll(done[2 * pair], HEAD, 1)
            both = jnp.where(lane < HEAD, even, done[2 * pair + 1]).astype(bf16)
            for k in range(out_ref.shape[0]):
                out_ref[k, at, pair * LANES : (pair + 1) * LANES] = both


def out_kernel(att_ref, w_ref, x_ref, rows_ref, out_ref, ready, sems):
    sources, n, _ = att_ref.shape
    t = lax.axis_index("tp")
    low = lanes_of((1, LANES)) < 64
    copies = []
    for i in range(n // REACH):
        at = slice(i * REACH, (i + 1) * REACH)
        att = jnp.concatenate([att_ref[k, at, :] for k in range(sources)], axis=1)
        mixed = jnp.dot(att, w_ref[...], preferred_element_type=f32)
        for m in range(out_ref.shape[1] // LANES):
            cols = slice(m * LANES, (m + 1) * LANES)
            a = rows_ref[t * 8 + 2 * m, 2:3, :]
            b = rows_ref[t * 8 + 2 * m + 1, 2:3, :]
            gate = jnp.where(low, a, pltpu.roll(b, 64, 1))
            ready[at, cols] = x_ref[at, cols].astype(f32) + gate * mixed[:, cols]
        copy = pltpu.make_async_copy(ready.at[at], out_ref.at[at], sems.at[i])
        copy.start()
        copies.append(copy)
    for copy in copies:
        copy.wait()


def rotary_table(places):
    lane = np.arange(LANES)
    freq = (ROTARY_BASE ** (-np.arange(0, 32, 2, dtype=np.float32) / 32)).astype(np.float32)
    angle = np.arange(places, dtype=np.float32)[:, None] * freq[lane % 16][None, :]
    sign = np.where(lane % 32 < 16, -1.0, 1.0)
    return np.stack([np.cos(angle), np.sin(angle) * sign[None, :]]).astype(np.float32)


def per_device(
    latent, conditioning, context_cond, modulation, context, query_weight, key_projection,
    value_projection, out_weight, sink_head_logit, prefix_logit_bias,
):
    sp, tp = lax.axis_size("sp"), lax.axis_size("tp")
    spread = tp * lax.axis_size("dp")
    x, ctx = latent[0], context[0]
    n = x.shape[0]
    partial = call(
        partial_kernel,
        jax.ShapeDtypeStruct((sp, PARTIAL_ROWS, LANES), bf16),
        [VMEM] * 3,
        [pltpu.VMEM((16, LANES), f32), pltpu.VMEM((PARTIAL_ROWS, LANES), f32)],
        56,
    )(conditioning, context_cond[None, :], modulation.transpose(0, 2, 1))
    with jax.named_scope("sums"):
        partials = lax.all_to_all(partial, "sp", 0, 0, tiled=True)
    flat = jax.ShapeDtypeStruct((n, LANES), f32)
    cflat = jax.ShapeDtypeStruct((ctx.shape[0], LANES), f32)
    mean, rstd, cmean, crstd = call(stats_kernel, (flat, flat, cflat, cflat), [VMEM] * 2, (), 8)(
        in_hbm(x), in_hbm(ctx)
    )
    wkv = jnp.concatenate([key_projection.T, value_projection.T], axis=0)
    by_row = jnp.asarray(rotary_table(sp * n // GRID_W))
    by_col = jnp.asarray(rotary_table(GRID_W))
    cols = out_weight.shape[1]
    own = lax.dynamic_slice_in_dim(x, lax.axis_index("tp") * cols, cols, 1)
    send = call(
        rows_kernel,
        jax.ShapeDtypeStruct((spread, 4, LANES), f32),
        [VMEM] + [ANY] * 3,
        [pltpu.VMEM((PARTIAL_ROWS, LANES), f32)],
        2,
    )(partials, cmean, wkv, own)
    with jax.named_scope("spread"):
        rows = lax.all_to_all(send, ("tp", "dp"), 0, 0, tiled=True)
    ctx_kv = call(
        ctx_kernel,
        jax.ShapeDtypeStruct((sp, ctx.shape[0], LANES), bf16),
        [VMEM] * 5,
        [],
        4,
    )(ctx, cmean, crstd, rows, wkv)
    with jax.named_scope("context"):
        ctx_all = lax.all_to_all(ctx_kv, "sp", 0, 0, tiled=True).reshape(-1, LANES)
    heads = query_weight.shape[1] // HEAD
    edge = jax.ShapeDtypeStruct((REACH, LANES), bf16)
    q, kv, first, last = call(
        project_kernel,
        (
            jax.ShapeDtypeStruct((heads, n, LANES), bf16),
            jax.ShapeDtypeStruct((n, LANES), bf16),
            edge,
            edge,
        ),
        [VMEM] * 8,
        [
            pltpu.VMEM(x.shape, bf16),
            pltpu.VMEM((n, LANES), f32),
            pltpu.VMEM((n, LANES), f32),
        ],
        7,
    )(in_hbm(x), mean, rstd, rows, in_hbm(query_weight), wkv, by_row, by_col)
    up = [(i, i + 1) for i in range(sp - 1)]
    down = [(i + 1, i) for i in range(sp - 1)]
    with jax.named_scope("halo"):
        before = lax.ppermute(last, "sp", up)
        after = lax.ppermute(first, "sp", down)
    wide = pltpu.VMEM((n + 2 * REACH, LANES), bf16)
    win = call(
        window_kernel,
        jax.ShapeDtypeStruct((heads, n, LANES), f32),
        [VMEM] * 4,
        [wide, wide],
        5,
    )(q, kv, before, after)
    attended = call(
        attend_kernel,
        jax.ShapeDtypeStruct((tp, n, heads * HEAD), bf16),
        [VMEM] * 3 + [SMEM] * 2 + [ANY],
        [pltpu.VMEM(ctx_all.shape, bf16)],
        8,
    )(q, win, ctx_all, sink_head_logit, prefix_logit_bias, out_weight)
    with jax.named_scope("heads"):
        every = lax.all_to_all(attended, "tp", 0, 0, tiled=True)
    out = call(
        out_kernel,
        pltpu.HBM((n, cols), f32),
        [VMEM] * 4,
        [pltpu.VMEM((n, cols), f32), pltpu.SemaphoreType.DMA((n // REACH,))],
        8,
        ANY,
    )(every, out_weight, own, rows)
    return out[None]


def solution(mesh):
    placed = (
        P("dp", "sp", None),
        P(None, "sp"),
        P("sp"),
        P(None, "sp", ("tp", "dp")),
        P("dp", "sp", None),
        P(None, "tp"),
        P(None, "tp"),
        P(None, "tp"),
        P(None, "tp"),
        P("tp"),
        P("tp"),
    )
    return jax.shard_map(
        per_device, mesh=mesh, in_specs=placed, out_specs=P("dp", "sp", "tp"), check_vma=False
    )
```

```python
import functools

import jax
import jax.numpy as jnp
import numpy as np
from jax import lax
from jax.experimental import pallas as pl
from jax.experimental.pallas import tpu as pltpu
from jax.sharding import PartitionSpec as P

HEAD = 64
GRID_W = 64
REACH = 128
EPS = 1e-06
ROTARY_BASE = 10000.0
MASKED = -1e30
LANES = 128
PARTIAL_ROWS = 24
GATE_ROWS = (9, 10, 11, 21)

f32 = jnp.float32
bf16 = jnp.bfloat16
VMEM = pl.BlockSpec(memory_space=pltpu.VMEM)
SMEM = pl.BlockSpec(memory_space=pltpu.SMEM)
ANY = pl.BlockSpec(memory_space=pl.ANY)


def in_hbm(x):
    return pltpu.with_memory_space_constraint(x, pltpu.HBM)


def dot_nt(a, b):
    return lax.dot_general(a, b, (((1,), (1,)), ((), ())), preferred_element_type=f32)


def lanes_of(shape):
    return lax.broadcasted_iota(jnp.int32, shape, len(shape) - 1)


def call(kernel, out_shape, ins, scratch=(), mib=8, out=VMEM, flags=None):
    return pl.pallas_call(
        kernel,
        out_shape=out_shape,
        in_specs=ins,
        out_specs=jax.tree.map(lambda _: out, out_shape),
        scratch_shapes=list(scratch),
        compiler_params=pltpu.CompilerParams(vmem_limit_bytes=mib << 20, flags=flags),
    )


def partial_kernel(cond_ref, ctx_ref, mod_ref, out_ref, rows, packed):
    samples = cond_ref.shape[0]
    rows[...] = jnp.zeros_like(rows)
    rows[0:samples, :] = cond_ref[...].astype(f32)
    rows[samples : samples + 1, :] = ctx_ref[...].astype(f32)
    v = rows[...]
    act = (v / (1.0 + jnp.exp(-v))).astype(bf16)
    shift = dot_nt(act, mod_ref[0])
    scale = dot_nt(act, mod_ref[1])
    gate = dot_nt(act, mod_ref[2])
    both = jnp.concatenate([shift, scale], axis=1)
    gates = jnp.concatenate([gate[0:4], gate[4:8]], axis=1)
    packed[...] = jnp.zeros_like(packed)
    packed[0:9, :] = both[0:9]
    packed[12:21, :] = (both - both.astype(bf16).astype(f32))[0:9]
    for j, row in enumerate(GATE_ROWS):
        packed[row : row + 1, :] = gates[j : j + 1]
    out_ref[...] = jnp.broadcast_to(packed[...].astype(bf16)[None], out_ref.shape)


def rows_kernel(in_ref, *refs):
    out_ref, total = refs[-2:]
    total[...] = jnp.sum(in_ref[...].astype(f32), axis=0)
    total[0:9, :] = total[0:9, :] + total[12:21, :]
    copies = out_ref.shape[0] // 8
    for d in range(8):
        row = GATE_ROWS[d % 4]
        gate = total[row : row + 1, :]
        if d >= 4:
            gate = pltpu.roll(gate, 64, 1)
        for t in range(copies):
            out_ref[t * 8 + d, 0:1, :] = total[d : d + 1, :]
            out_ref[t * 8 + d, 1:2, :] = total[8:9, :]
            out_ref[t * 8 + d, 2:3, :] = gate
            out_ref[t * 8 + d, 3:4, :] = gate


def stats_of(x_ref, mean_ref, rstd_ref):
    width = x_ref.shape[1]
    step = 64

    def body(i, carry):
        at = pl.ds(pl.multiple_of(i * step, step), step)
        x = x_ref[at, :].astype(f32)
        mean = jnp.sum(x, axis=1, keepdims=True) * (1.0 / width)
        d = x - mean
        var = jnp.sum(d * d, axis=1, keepdims=True) * (1.0 / width)
        mean_ref[at, :] = jnp.broadcast_to(mean, (step, LANES))
        rstd_ref[at, :] = jnp.broadcast_to(lax.rsqrt(var + EPS), (step, LANES))
        return carry

    lax.fori_loop(0, x_ref.shape[0] // step, body, 0)


def stats_kernel(x_ref, c_ref, mean_ref, rstd_ref, cmean_ref, crstd_ref):
    stats_of(x_ref, mean_ref, rstd_ref)
    stats_of(c_ref, cmean_ref, crstd_ref)


def mod_tile(rows_ref, row, m):
    a = rows_ref[2 * m, row : row + 1, :]
    b = rows_ref[2 * m + 1, row : row + 1, :]
    low = lanes_of((1, LANES)) < 64
    shift = jnp.where(low, a, pltpu.roll(b, 64, 1))
    scale = jnp.where(low, pltpu.roll(a, 64, 1), b)
    return shift, 1.0 + scale


def modulate(x_ref, mean_ref, rstd_ref, rows_ref, row, out_ref, start):
    n = x_ref.shape[0]
    for m in range(x_ref.shape[1] // LANES):
        shift, scale = mod_tile(rows_ref, row, m)
        cols = slice(m * LANES, (m + 1) * LANES)
        x = x_ref[:, cols].astype(f32)
        y = (x - mean_ref[...]) * rstd_ref[...] * scale + shift
        out_ref[start : start + n, cols] = y.astype(bf16)


def ctx_kernel(x_ref, mean_ref, rstd_ref, rows_ref, wkv_ref, out_ref):
    acc = jnp.zeros((x_ref.shape[0], LANES), f32)
    for m in range(0, x_ref.shape[1] // LANES, 2):
        parts = []
        for k in (m, m + 1):
            shift, scale = mod_tile(rows_ref, 1, k)
            x = x_ref[:, k * LANES : (k + 1) * LANES].astype(f32)
            y = (x - mean_ref[...]) * rstd_ref[...] * scale + shift
            parts.append(y.astype(bf16))
        wide = slice(m * LANES, (m + 2) * LANES)
        acc = acc + dot_nt(jnp.concatenate(parts, axis=1), wkv_ref[:, wide])
    out_ref[...] = jnp.broadcast_to(acc.astype(bf16)[None], out_ref.shape)


def turned(u, cos, sin):
    low = lanes_of(u.shape) % 32 < 16
    other = jnp.where(low, pltpu.roll(u, LANES - 16, 1), pltpu.roll(u, 16, 1))
    return u * cos + other * sin


def with_ones(kv):
    return jnp.where(lanes_of(kv.shape) < HEAD, jnp.ones_like(kv), kv)


def project_kernel(
    x_ref, mean_ref, rstd_ref, rows_ref, wq_ref, wkv_ref, row_ref, col_ref,
    q_ref, kv_ref, head_ref, tail_ref, normed, cos_s, sin_s,
):
    n = x_ref.shape[0]
    modulate(x_ref, mean_ref, rstd_ref, rows_ref, 0, normed, 0)
    by_row = lanes_of((GRID_W, LANES)) % HEAD < HEAD // 2
    first = lax.axis_index("sp") * (n // GRID_W)
    for g in range(n // GRID_W):
        at = slice(g * GRID_W, (g + 1) * GRID_W)
        cos_s[at, :] = jnp.where(by_row, row_ref[0, pl.ds(first + g, 1), :], col_ref[0])
        sin_s[at, :] = jnp.where(by_row, row_ref[1, pl.ds(first + g, 1), :], col_ref[1])
    cos, sin = cos_s[...], sin_s[...]
    low = lanes_of((n, LANES)) < HEAD
    kv = dot_nt(normed[...], wkv_ref[...])
    kv = turned(kv, jnp.where(low, cos, 1.0), jnp.where(low, sin, 0.0)).astype(bf16)
    kv_ref[...] = kv
    head_ref[...] = kv[0:REACH]
    tail_ref[...] = kv[n - REACH : n]
    q = jnp.dot(normed[...], wq_ref[...], preferred_element_type=f32)
    for pair in range(q.shape[1] // LANES):
        u = turned(q[:, pair * LANES : (pair + 1) * LANES], cos, sin) * (HEAD ** -0.5)
        q_ref[2 * pair] = jnp.where(low, u, 0.0).astype(bf16)
        q_ref[2 * pair + 1] = jnp.where(low, pltpu.roll(u, HEAD, 1), 0.0).astype(bf16)


def window_kernel(q_ref, kv_ref, before_ref, after_ref, win_ref, kv_s, ones_s):
    heads, n, _ = q_ref.shape
    kv_s[0:REACH, :] = before_ref[...]
    kv_s[REACH : REACH + n, :] = kv_ref[...]
    kv_s[REACH + n :, :] = after_ref[...]
    ones_s[...] = with_ones(kv_s[...])
    rows = heads * REACH
    blocks = n // REACH
    i = lax.broadcasted_iota(jnp.int32, (rows, 3 * REACH), 0) % REACH
    j = lanes_of((rows, 3 * REACH))
    near = (j >= i) & (j <= i + 2 * REACH)
    place = lax.axis_index("sp")
    first, last = place == 0, place == lax.axis_size("sp") - 1
    for b in range(blocks):
        qb = q_ref[:, b * REACH : (b + 1) * REACH, :].reshape(rows, LANES)
        s = dot_nt(qb, kv_s[b * REACH : (b + 3) * REACH, :])
        valid = near
        if b == 0:
            valid = valid & (j >= jnp.where(first, REACH, 0))
        if b == blocks - 1:
            valid = valid & (j < jnp.where(last, 2 * REACH, 3 * REACH))
        s = jnp.where(valid, s, MASKED)
        top = jnp.max(s, axis=1, keepdims=True)
        p = jnp.exp(s - top).astype(bf16)
        acc = jnp.dot(p, ones_s[b * REACH : (b + 3) * REACH, :], preferred_element_type=f32)
        acc = jnp.where(lanes_of(acc.shape) == 0, top, acc)
        win_ref[:, b * REACH : (b + 1) * REACH, :] = acc.reshape(heads, REACH, LANES)


def top_of(s):
    m = s[:, 0:LANES]
    for k in range(1, s.shape[1] // LANES):
        m = jnp.maximum(m, s[:, k * LANES : (k + 1) * LANES])
    return jnp.max(m, axis=1, keepdims=True)


def attend_kernel(q_ref, win_ref, ctx_ref, sink_ref, bias_ref, _, out_ref, ones_s):
    heads, n, _ = q_ref.shape
    lane = lanes_of((REACH, LANES))

    sub = 2
    rows = sub * REACH
    def part(x, fill):
        head = lax.broadcasted_iota(jnp.int32, (rows, 1), 0) // REACH
        out = jnp.zeros((rows, 1), f32)
        for h in range(sub):
            out = jnp.where(head == h, x[fill + h], out)
        return out
    units = [(b, g) for b in range(n // REACH) for g in range(heads // sub)]
    biases = [part(bias_ref, g * sub) for g in range(heads // sub)]
    sinks = [part(sink_ref, g * sub) for g in range(heads // sub)]
    def score(u):
        b, g = u
        at = slice(b * REACH, (b + 1) * REACH)
        q = q_ref[g * sub : (g + 1) * sub, at, :].reshape(rows, LANES)
        return dot_nt(q, ctx_ref[...])
    ahead = 2
    queue = [score(u) for u in units[:ahead]]
    ones_s[...] = with_ones(ctx_ref[...])
    done = []
    for i, (b, g) in enumerate(units):
        if ahead == 0:
            s = score((b, g))
        else:
            s = queue.pop(0)
            if i + ahead < len(units):
                queue.append(score(units[i + ahead]))
        at = slice(b * REACH, (b + 1) * REACH)
        win = win_ref[g * sub : (g + 1) * sub, at, :].reshape(rows, LANES)
        win_top = win[:, 0:1]
        bias, sink = biases[g], sinks[g]
        top = jnp.maximum(top_of(s) + bias, jnp.maximum(win_top, sink))
        p = jnp.exp(s - (top - bias)).astype(bf16)
        acc = jnp.dot(p, ones_s[...], preferred_element_type=f32) + win * jnp.exp(win_top - top)
        acc = (acc * (1.0 / (acc[:, 1:2] + jnp.exp(sink - top)))).reshape(sub, REACH, LANES)
        if g == 0:
            done = []
        done.extend(acc[h] for h in range(sub))
        if g < heads // sub - 1:
            continue

        for pair in range(heads // 2):
            even = pltpu.roll(done[2 * pair], HEAD, 1)
            both = jnp.where(lane < HEAD, even, done[2 * pair + 1]).astype(bf16)
            for k in range(out_ref.shape[0]):
                out_ref[k, at, pair * LANES : (pair + 1) * LANES] = both


def out_kernel(att_ref, w_ref, x_ref, rows_ref, out_ref, ready, sems):
    sources, n, _ = att_ref.shape
    t = lax.axis_index("tp")
    low = lanes_of((1, LANES)) < 64
    copies = []
    for i in range(n // REACH):
        at = slice(i * REACH, (i + 1) * REACH)
        att = jnp.concatenate([att_ref[k, at, :] for k in range(sources)], axis=1)
        mixed = jnp.dot(att, w_ref[...], preferred_element_type=f32)
        for m in range(out_ref.shape[1] // LANES):
            cols = slice(m * LANES, (m + 1) * LANES)
            a = rows_ref[t * 8 + 2 * m, 2:3, :]
            b = rows_ref[t * 8 + 2 * m + 1, 2:3, :]
            gate = jnp.where(low, a, pltpu.roll(b, 64, 1))
            ready[at, cols] = x_ref[at, cols].astype(f32) + gate * mixed[:, cols]
        copy = pltpu.make_async_copy(ready.at[at], out_ref.at[at], sems.at[i])
        copy.start()
        copies.append(copy)
    for copy in copies:
        copy.wait()


def rotary_table(places):
    lane = np.arange(LANES)
    freq = (ROTARY_BASE ** (-np.arange(0, 32, 2, dtype=np.float32) / 32)).astype(np.float32)
    angle = np.arange(places, dtype=np.float32)[:, None] * freq[lane % 16][None, :]
    sign = np.where(lane % 32 < 16, -1.0, 1.0)
    return np.stack([np.cos(angle), np.sin(angle) * sign[None, :]]).astype(np.float32)


def per_device(
    latent, conditioning, context_cond, modulation, context, query_weight, key_projection,
    value_projection, out_weight, sink_head_logit, prefix_logit_bias,
):
    sp, tp = lax.axis_size("sp"), lax.axis_size("tp")
    spread = tp * lax.axis_size("dp")
    x, ctx = latent[0], context[0]
    n = x.shape[0]
    partial = call(
        partial_kernel,
        jax.ShapeDtypeStruct((sp, PARTIAL_ROWS, LANES), bf16),
        [VMEM] * 3,
        [pltpu.VMEM((16, LANES), f32), pltpu.VMEM((PARTIAL_ROWS, LANES), f32)],
        56,
    )(conditioning, context_cond[None, :], modulation.transpose(0, 2, 1))
    with jax.named_scope("sums"):
        partials = lax.all_to_all(partial, "sp", 0, 0, tiled=True)
    flat = jax.ShapeDtypeStruct((n, LANES), f32)
    cflat = jax.ShapeDtypeStruct((ctx.shape[0], LANES), f32)
    mean, rstd, cmean, crstd = call(stats_kernel, (flat, flat, cflat, cflat), [VMEM] * 2, (), 8)(
        in_hbm(x), in_hbm(ctx)
    )
    wkv = jnp.concatenate([key_projection.T, value_projection.T], axis=0)
    by_row = jnp.asarray(rotary_table(sp * n // GRID_W))
    by_col = jnp.asarray(rotary_table(GRID_W))
    cols = out_weight.shape[1]
    own = lax.dynamic_slice_in_dim(x, lax.axis_index("tp") * cols, cols, 1)
    send = call(
        rows_kernel,
        jax.ShapeDtypeStruct((spread, 4, LANES), f32),
        [VMEM] + [ANY] * 3,
        [pltpu.VMEM((PARTIAL_ROWS, LANES), f32)],
        2,
    )(partials, cmean, wkv, own)
    with jax.named_scope("spread"):
        rows = lax.all_to_all(send, ("tp", "dp"), 0, 0, tiled=True)
    ctx_kv = call(
        ctx_kernel,
        jax.ShapeDtypeStruct((sp, ctx.shape[0], LANES), bf16),
        [VMEM] * 5,
        [],
        4,
    )(ctx, cmean, crstd, rows, wkv)
    with jax.named_scope("context"):
        ctx_all = lax.all_to_all(ctx_kv, "sp", 0, 0, tiled=True).reshape(-1, LANES)
    heads = query_weight.shape[1] // HEAD
    edge = jax.ShapeDtypeStruct((REACH, LANES), bf16)
    q, kv, first, last = call(
        project_kernel,
        (
            jax.ShapeDtypeStruct((heads, n, LANES), bf16),
            jax.ShapeDtypeStruct((n, LANES), bf16),
            edge,
            edge,
        ),
        [VMEM] * 8,
        [
            pltpu.VMEM(x.shape, bf16),
            pltpu.VMEM((n, LANES), f32),
            pltpu.VMEM((n, LANES), f32),
        ],
        7,
    )(in_hbm(x), mean, rstd, rows, in_hbm(query_weight), wkv, by_row, by_col)
    up = [(i, i + 1) for i in range(sp - 1)]
    down = [(i + 1, i) for i in range(sp - 1)]
    with jax.named_scope("halo"):
        before = lax.ppermute(last, "sp", up)
        after = lax.ppermute(first, "sp", down)
    wide = pltpu.VMEM((n + 2 * REACH, LANES), bf16)
    win = call(
        window_kernel,
        jax.ShapeDtypeStruct((heads, n, LANES), f32),
        [VMEM] * 4,
        [wide, wide],
        5,
    )(q, kv, before, after)
    attended = call(
        attend_kernel,
        jax.ShapeDtypeStruct((tp, n, heads * HEAD), bf16),
        [VMEM] * 3 + [SMEM] * 2 + [ANY],
        [pltpu.VMEM(ctx_all.shape, bf16)],
        8,
    )(q, win, ctx_all, sink_head_logit, prefix_logit_bias, out_weight)
    with jax.named_scope("heads"):
        every = lax.all_to_all(attended, "tp", 0, 0, tiled=True)
    out = call(
        out_kernel,
        pltpu.HBM((n, cols), f32),
        [VMEM] * 4,
        [pltpu.VMEM((n, cols), f32), pltpu.SemaphoreType.DMA((n // REACH,))],
        8,
        ANY,
    )(every, out_weight, own, rows)
    return out[None]


def solution(mesh):
    placed = (
        P("dp", "sp", None),
        P(None, "sp"),
        P("sp"),
        P(None, "sp", ("tp", "dp")),
        P("dp", "sp", None),
        P(None, "tp"),
        P(None, "tp"),
        P(None, "tp"),
        P(None, "tp"),
        P("tp"),
        P("tp"),
    )
    return jax.shard_map(
        per_device, mesh=mesh, in_specs=placed, out_specs=P("dp", "sp", "tp"), check_vma=False
    )
```

```python
import functools

import jax
import jax.numpy as jnp
import numpy as np
from jax import lax
from jax.experimental import pallas as pl
from jax.experimental.pallas import tpu as pltpu
from jax.sharding import PartitionSpec as P

HEAD = 64
GRID_W = 64
REACH = 128
EPS = 1e-06
ROTARY_BASE = 10000.0
MASKED = -1e30
LANES = 128
PARTIAL_ROWS = 24
GATE_ROWS = (9, 10, 11, 21)

f32 = jnp.float32
bf16 = jnp.bfloat16
VMEM = pl.BlockSpec(memory_space=pltpu.VMEM)
SMEM = pl.BlockSpec(memory_space=pltpu.SMEM)
ANY = pl.BlockSpec(memory_space=pl.ANY)


def in_hbm(x):
    return pltpu.with_memory_space_constraint(x, pltpu.HBM)


def dot_nt(a, b):
    return lax.dot_general(a, b, (((1,), (1,)), ((), ())), preferred_element_type=f32)


def lanes_of(shape):
    return lax.broadcasted_iota(jnp.int32, shape, len(shape) - 1)


def call(kernel, out_shape, ins, scratch=(), mib=8, out=VMEM, flags=None):
    return pl.pallas_call(
        kernel,
        out_shape=out_shape,
        in_specs=ins,
        out_specs=jax.tree.map(lambda _: out, out_shape),
        scratch_shapes=list(scratch),
        compiler_params=pltpu.CompilerParams(vmem_limit_bytes=mib << 20, flags=flags),
    )


def partial_kernel(cond_ref, ctx_ref, mod_ref, out_ref, rows, packed):
    samples = cond_ref.shape[0]
    rows[...] = jnp.zeros_like(rows)
    rows[0:samples, :] = cond_ref[...].astype(f32)
    rows[samples : samples + 1, :] = ctx_ref[...].astype(f32)
    v = rows[...]
    act = (v / (1.0 + jnp.exp(-v))).astype(bf16)
    shift = dot_nt(act, mod_ref[0])
    scale = dot_nt(act, mod_ref[1])
    gate = dot_nt(act, mod_ref[2])
    both = jnp.concatenate([shift, scale], axis=1)
    gates = jnp.concatenate([gate[0:4], gate[4:8]], axis=1)
    packed[...] = jnp.zeros_like(packed)
    packed[0:9, :] = both[0:9]
    packed[12:21, :] = (both - both.astype(bf16).astype(f32))[0:9]
    for j, row in enumerate(GATE_ROWS):
        packed[row : row + 1, :] = gates[j : j + 1]
    out_ref[...] = jnp.broadcast_to(packed[...].astype(bf16)[None], out_ref.shape)


def rows_kernel(in_ref, *refs):
    out_ref, total = refs[-2:]
    total[...] = jnp.sum(in_ref[...].astype(f32), axis=0)
    total[0:9, :] = total[0:9, :] + total[12:21, :]
    copies = out_ref.shape[0] // 8
    for d in range(8):
        row = GATE_ROWS[d % 4]
        gate = total[row : row + 1, :]
        if d >= 4:
            gate = pltpu.roll(gate, 64, 1)
        for t in range(copies):
            out_ref[t * 8 + d, 0:1, :] = total[d : d + 1, :]
            out_ref[t * 8 + d, 1:2, :] = total[8:9, :]
            out_ref[t * 8 + d, 2:3, :] = gate
            out_ref[t * 8 + d, 3:4, :] = gate


def stats_of(x_ref, mean_ref, rstd_ref):
    width = x_ref.shape[1]
    step = 64

    def body(i, carry):
        at = pl.ds(pl.multiple_of(i * step, step), step)
        x = x_ref[at, :].astype(f32)
        mean = jnp.sum(x, axis=1, keepdims=True) * (1.0 / width)
        d = x - mean
        var = jnp.sum(d * d, axis=1, keepdims=True) * (1.0 / width)
        mean_ref[at, :] = jnp.broadcast_to(mean, (step, LANES))
        rstd_ref[at, :] = jnp.broadcast_to(lax.rsqrt(var + EPS), (step, LANES))
        return carry

    lax.fori_loop(0, x_ref.shape[0] // step, body, 0)


def stats_kernel(x_ref, c_ref, mean_ref, rstd_ref, cmean_ref, crstd_ref):
    stats_of(x_ref, mean_ref, rstd_ref)
    stats_of(c_ref, cmean_ref, crstd_ref)


def mod_tile(rows_ref, row, m):
    a = rows_ref[2 * m, row : row + 1, :]
    b = rows_ref[2 * m + 1, row : row + 1, :]
    low = lanes_of((1, LANES)) < 64
    shift = jnp.where(low, a, pltpu.roll(b, 64, 1))
    scale = jnp.where(low, pltpu.roll(a, 64, 1), b)
    return shift, 1.0 + scale


def modulate(x_ref, mean_ref, rstd_ref, rows_ref, row, out_ref, start):
    n = x_ref.shape[0]
    for m in range(x_ref.shape[1] // LANES):
        shift, scale = mod_tile(rows_ref, row, m)
        cols = slice(m * LANES, (m + 1) * LANES)
        x = x_ref[:, cols].astype(f32)
        y = (x - mean_ref[...]) * rstd_ref[...] * scale + shift
        out_ref[start : start + n, cols] = y.astype(bf16)


def ctx_kernel(x_ref, mean_ref, rstd_ref, rows_ref, wkv_ref, out_ref):
    acc = jnp.zeros((x_ref.shape[0], LANES), f32)
    for m in range(0, x_ref.shape[1] // LANES, 2):
        parts = []
        for k in (m, m + 1):
            shift, scale = mod_tile(rows_ref, 1, k)
            x = x_ref[:, k * LANES : (k + 1) * LANES].astype(f32)
            y = (x - mean_ref[...]) * rstd_ref[...] * scale + shift
            parts.append(y.astype(bf16))
        wide = slice(m * LANES, (m + 2) * LANES)
        acc = acc + dot_nt(jnp.concatenate(parts, axis=1), wkv_ref[:, wide])
    out_ref[...] = jnp.broadcast_to(acc.astype(bf16)[None], out_ref.shape)


def turned(u, cos, sin):
    low = lanes_of(u.shape) % 32 < 16
    other = jnp.where(low, pltpu.roll(u, LANES - 16, 1), pltpu.roll(u, 16, 1))
    return u * cos + other * sin


def with_ones(kv):
    return jnp.where(lanes_of(kv.shape) < HEAD, jnp.ones_like(kv), kv)


def project_kernel(
    x_ref, mean_ref, rstd_ref, rows_ref, wq_ref, wkv_ref, row_ref, col_ref,
    q_ref, kv_ref, head_ref, tail_ref, normed, cos_s, sin_s,
):
    n = x_ref.shape[0]
    modulate(x_ref, mean_ref, rstd_ref, rows_ref, 0, normed, 0)
    by_row = lanes_of((GRID_W, LANES)) % HEAD < HEAD // 2
    first = lax.axis_index("sp") * (n // GRID_W)
    for g in range(n // GRID_W):
        at = slice(g * GRID_W, (g + 1) * GRID_W)
        cos_s[at, :] = jnp.where(by_row, row_ref[0, pl.ds(first + g, 1), :], col_ref[0])
        sin_s[at, :] = jnp.where(by_row, row_ref[1, pl.ds(first + g, 1), :], col_ref[1])
    cos, sin = cos_s[...], sin_s[...]
    low = lanes_of((n, LANES)) < HEAD
    kv = dot_nt(normed[...], wkv_ref[...])
    kv = turned(kv, jnp.where(low, cos, 1.0), jnp.where(low, sin, 0.0)).astype(bf16)
    kv_ref[...] = kv
    head_ref[...] = kv[0:REACH]
    tail_ref[...] = kv[n - REACH : n]
    q = jnp.dot(normed[...], wq_ref[...], preferred_element_type=f32)
    for pair in range(q.shape[1] // LANES):
        u = turned(q[:, pair * LANES : (pair + 1) * LANES], cos, sin) * (HEAD ** -0.5)
        q_ref[2 * pair] = jnp.where(low, u, 0.0).astype(bf16)
        q_ref[2 * pair + 1] = jnp.where(low, pltpu.roll(u, HEAD, 1), 0.0).astype(bf16)


def window_kernel(q_ref, kv_ref, before_ref, after_ref, win_ref, kv_s, ones_s):
    heads, n, _ = q_ref.shape
    kv_s[0:REACH, :] = before_ref[...]
    kv_s[REACH : REACH + n, :] = kv_ref[...]
    kv_s[REACH + n :, :] = after_ref[...]
    ones_s[...] = with_ones(kv_s[...])
    rows = heads * REACH
    blocks = n // REACH
    i = lax.broadcasted_iota(jnp.int32, (rows, 3 * REACH), 0) % REACH
    j = lanes_of((rows, 3 * REACH))
    near = (j >= i) & (j <= i + 2 * REACH)
    place = lax.axis_index("sp")
    first, last = place == 0, place == lax.axis_size("sp") - 1
    for b in range(blocks):
        qb = q_ref[:, b * REACH : (b + 1) * REACH, :].reshape(rows, LANES)
        s = dot_nt(qb, kv_s[b * REACH : (b + 3) * REACH, :])
        valid = near
        if b == 0:
            valid = valid & (j >= jnp.where(first, REACH, 0))
        if b == blocks - 1:
            valid = valid & (j < jnp.where(last, 2 * REACH, 3 * REACH))
        s = jnp.where(valid, s, MASKED)
        top = jnp.max(s, axis=1, keepdims=True)
        p = jnp.exp(s - top).astype(bf16)
        acc = jnp.dot(p, ones_s[b * REACH : (b + 3) * REACH, :], preferred_element_type=f32)
        acc = jnp.where(lanes_of(acc.shape) == 0, top, acc)
        win_ref[:, b * REACH : (b + 1) * REACH, :] = acc.reshape(heads, REACH, LANES)


def top_of(s):
    m = s[:, 0:LANES]
    for k in range(1, s.shape[1] // LANES):
        m = jnp.maximum(m, s[:, k * LANES : (k + 1) * LANES])
    return jnp.max(m, axis=1, keepdims=True)


def attend_kernel(q_ref, win_ref, ctx_ref, sink_ref, bias_ref, _, out_ref, ones_s):
    heads, n, _ = q_ref.shape
    lane = lanes_of((REACH, LANES))

    sub = 2
    rows = sub * REACH
    def part(x, fill):
        head = lax.broadcasted_iota(jnp.int32, (rows, 1), 0) // REACH
        out = jnp.zeros((rows, 1), f32)
        for h in range(sub):
            out = jnp.where(head == h, x[fill + h], out)
        return out
    units = [(b, g) for b in range(n // REACH) for g in range(heads // sub)]
    biases = [part(bias_ref, g * sub) for g in range(heads // sub)]
    sinks = [part(sink_ref, g * sub) for g in range(heads // sub)]
    def score(u):
        b, g = u
        at = slice(b * REACH, (b + 1) * REACH)
        q = q_ref[g * sub : (g + 1) * sub, at, :].reshape(rows, LANES)
        return dot_nt(q, ctx_ref[...])
    ahead = 2
    queue = [score(u) for u in units[:ahead]]
    ones_s[...] = with_ones(ctx_ref[...])
    done = []
    for i, (b, g) in enumerate(units):
        if ahead == 0:
            s = score((b, g))
        else:
            s = queue.pop(0)
            if i + ahead < len(units):
                queue.append(score(units[i + ahead]))
        at = slice(b * REACH, (b + 1) * REACH)
        win = win_ref[g * sub : (g + 1) * sub, at, :].reshape(rows, LANES)
        win_top = win[:, 0:1]
        bias, sink = biases[g], sinks[g]
        top = jnp.maximum(top_of(s) + bias, jnp.maximum(win_top, sink))
        p = jnp.exp(s - (top - bias)).astype(bf16)
        acc = jnp.dot(p, ones_s[...], preferred_element_type=f32) + win * jnp.exp(win_top - top)
        acc = (acc * (1.0 / (acc[:, 1:2] + jnp.exp(sink - top)))).reshape(sub, REACH, LANES)
        if g == 0:
            done = []
        done.extend(acc[h] for h in range(sub))
        if g < heads // sub - 1:
            continue

        for pair in range(heads // 2):
            even = pltpu.roll(done[2 * pair], HEAD, 1)
            both = jnp.where(lane < HEAD, even, done[2 * pair + 1]).astype(bf16)
            for k in range(out_ref.shape[0]):
                out_ref[k, at, pair * LANES : (pair + 1) * LANES] = both


def out_kernel(att_ref, w_ref, x_ref, rows_ref, out_ref, ready, sems):
    sources, n, _ = att_ref.shape
    t = lax.axis_index("tp")
    low = lanes_of((1, LANES)) < 64
    gates = []
    for m in range(out_ref.shape[1] // LANES):
        a = rows_ref[t * 8 + 2 * m, 2:3, :]
        b = rows_ref[t * 8 + 2 * m + 1, 2:3, :]
        gates.append(jnp.where(low, a, pltpu.roll(b, 64, 1)))
    copies = []
    for i in range(n // REACH):
        at = slice(i * REACH, (i + 1) * REACH)
        att = jnp.concatenate([att_ref[k, at, :] for k in range(sources)], axis=1)
        mixed = jnp.dot(att, w_ref[...], preferred_element_type=f32)
        for m in range(out_ref.shape[1] // LANES):
            cols = slice(m * LANES, (m + 1) * LANES)
            ready[at, cols] = x_ref[at, cols].astype(f32) + gates[m] * mixed[:, cols]
        copy = pltpu.make_async_copy(ready.at[at], out_ref.at[at], sems.at[i])
        copy.start()
        copies.append(copy)
    for copy in copies:
        copy.wait()


def rotary_table(places):
    lane = np.arange(LANES)
    freq = (ROTARY_BASE ** (-np.arange(0, 32, 2, dtype=np.float32) / 32)).astype(np.float32)
    angle = np.arange(places, dtype=np.float32)[:, None] * freq[lane % 16][None, :]
    sign = np.where(lane % 32 < 16, -1.0, 1.0)
    return np.stack([np.cos(angle), np.sin(angle) * sign[None, :]]).astype(np.float32)


def per_device(
    latent, conditioning, context_cond, modulation, context, query_weight, key_projection,
    value_projection, out_weight, sink_head_logit, prefix_logit_bias,
):
    sp, tp = lax.axis_size("sp"), lax.axis_size("tp")
    spread = tp * lax.axis_size("dp")
    x, ctx = latent[0], context[0]
    n = x.shape[0]
    partial = call(
        partial_kernel,
        jax.ShapeDtypeStruct((sp, PARTIAL_ROWS, LANES), bf16),
        [VMEM] * 3,
        [pltpu.VMEM((16, LANES), f32), pltpu.VMEM((PARTIAL_ROWS, LANES), f32)],
        56,
    )(conditioning, context_cond[None, :], modulation.transpose(0, 2, 1))
    with jax.named_scope("sums"):
        partials = lax.all_to_all(partial, "sp", 0, 0, tiled=True)
    flat = jax.ShapeDtypeStruct((n, LANES), f32)
    cflat = jax.ShapeDtypeStruct((ctx.shape[0], LANES), f32)
    mean, rstd, cmean, crstd = call(stats_kernel, (flat, flat, cflat, cflat), [VMEM] * 2, (), 8)(
        in_hbm(x), in_hbm(ctx)
    )
    wkv = jnp.concatenate([key_projection.T, value_projection.T], axis=0)
    by_row = jnp.asarray(rotary_table(sp * n // GRID_W))
    by_col = jnp.asarray(rotary_table(GRID_W))
    cols = out_weight.shape[1]
    own = lax.dynamic_slice_in_dim(x, lax.axis_index("tp") * cols, cols, 1)
    send = call(
        rows_kernel,
        jax.ShapeDtypeStruct((spread, 4, LANES), f32),
        [VMEM] + [ANY] * 3,
        [pltpu.VMEM((PARTIAL_ROWS, LANES), f32)],
        2,
    )(partials, cmean, wkv, own)
    with jax.named_scope("spread"):
        rows = lax.all_to_all(send, ("tp", "dp"), 0, 0, tiled=True)
    ctx_kv = call(
        ctx_kernel,
        jax.ShapeDtypeStruct((sp, ctx.shape[0], LANES), bf16),
        [VMEM] * 5,
        [],
        4,
    )(ctx, cmean, crstd, rows, wkv)
    with jax.named_scope("context"):
        ctx_all = lax.all_to_all(ctx_kv, "sp", 0, 0, tiled=True).reshape(-1, LANES)
    heads = query_weight.shape[1] // HEAD
    edge = jax.ShapeDtypeStruct((REACH, LANES), bf16)
    q, kv, first, last = call(
        project_kernel,
        (
            jax.ShapeDtypeStruct((heads, n, LANES), bf16),
            jax.ShapeDtypeStruct((n, LANES), bf16),
            edge,
            edge,
        ),
        [VMEM] * 8,
        [
            pltpu.VMEM(x.shape, bf16),
            pltpu.VMEM((n, LANES), f32),
            pltpu.VMEM((n, LANES), f32),
        ],
        7,
    )(in_hbm(x), mean, rstd, rows, in_hbm(query_weight), wkv, by_row, by_col)
    up = [(i, i + 1) for i in range(sp - 1)]
    down = [(i + 1, i) for i in range(sp - 1)]
    with jax.named_scope("halo"):
        before = lax.ppermute(last, "sp", up)
        after = lax.ppermute(first, "sp", down)
    wide = pltpu.VMEM((n + 2 * REACH, LANES), bf16)
    win = call(
        window_kernel,
        jax.ShapeDtypeStruct((heads, n, LANES), f32),
        [VMEM] * 4,
        [wide, wide],
        5,
    )(q, kv, before, after)
    attended = call(
        attend_kernel,
        jax.ShapeDtypeStruct((tp, n, heads * HEAD), bf16),
        [VMEM] * 3 + [SMEM] * 2 + [ANY],
        [pltpu.VMEM(ctx_all.shape, bf16)],
        8,
    )(q, win, ctx_all, sink_head_logit, prefix_logit_bias, out_weight)
    with jax.named_scope("heads"):
        every = lax.all_to_all(attended, "tp", 0, 0, tiled=True)
    out = call(
        out_kernel,
        pltpu.HBM((n, cols), f32),
        [VMEM] * 4,
        [pltpu.VMEM((n, cols), f32), pltpu.SemaphoreType.DMA((n // REACH,))],
        8,
        ANY,
    )(every, out_weight, own, rows)
    return out[None]


def solution(mesh):
    placed = (
        P("dp", "sp", None),
        P(None, "sp"),
        P("sp"),
        P(None, "sp", ("tp", "dp")),
        P("dp", "sp", None),
        P(None, "tp"),
        P(None, "tp"),
        P(None, "tp"),
        P(None, "tp"),
        P("tp"),
        P("tp"),
    )
    return jax.shard_map(
        per_device, mesh=mesh, in_specs=placed, out_specs=P("dp", "sp", "tp"), check_vma=False
    )
```
